128 devices in a mesh: sp: 16 (over z, y), tp: 8 (over x, core).
Axes of the slice: x: 4, y: 4, z: 4, core: 2. Of those that a mesh axis runs over, the one named last changes fastest.
Arguments:
- stream: bfloat16 [6144, 2048], P(('sp', 'tp')), may hold values from -6 to 6
- query_nope: bfloat16 [6144, 16, 128], P('sp', 'tp'), may hold values from -6 to 6
- query_rope: bfloat16 [6144, 16, 64], P('sp', 'tp'), may hold values from -700 to 700
- latent: bfloat16 [6144, 512], P('sp'), may hold values from -6 to 6
- rope_key: bfloat16 [6144, 64], P('sp'), may hold values from -6 to 6
- latent_gain: float32 [512], replicated, may hold values from 0.1 to 1.9
- key_up: bfloat16 [512, 16, 128], P(None, 'tp'), may hold values from -0.375 to 0.375
- value_up: bfloat16 [512, 16, 128], P(None, 'tp'), may hold values from -2.6516504 to 2.6516504
- out_gain: float32 [2048], P('tp'), may hold values from 0.1 to 1.9
- out_weight: bfloat16 [2048, 2048], P('tp'), may hold values from -0.125 to 0.125
- norm_gain: float32 [2048], replicated, may hold values from 0.1 to 1.9
- ff_in: bfloat16 [2048, 8192], P('sp', 'tp'), may hold values from -0.125 to 0.125
- ff_out: bfloat16 [8192, 2048], P('tp', 'sp'), may hold values from -0.0625 to 0.0625
Outputs:
- layer_out: bfloat16 [6144, 2048], P(('sp', 'tp'))
The draws below stay inside these ranges and needn't reach their ends.
All inputs are finite; a program needn't handle non-finite values.
Results may differ from the reference program's by a relative error of at most 0.018.
Values may be sent and summed in bfloat16 or wider, within the bound.
No kernel may reach another device: no remote copies, remote signals or barrier semaphores. Data moves between devices by JAX's collectives and lax.ppermute only.
A program may use at most 128 MiB of HBM per device.

```python
import math
import jax
import jax.numpy as jnp
from jax import lax

D = 2048
FF = 8192
HEADS = 16
NOPE = 128
ROPE = 64
LATENT = 512
VDIM = 128
TOKENS = 6144


def draw_query_rope(key, part):
    base_draw = jax.random.normal(key, (TOKENS, HEADS, ROPE), jnp.float32)
    return jnp.clip(base_draw, -700.0, 700.0).astype(jnp.bfloat16)


def draw_value_up(key, part):
    base_draw = jnp.clip(jax.random.normal(key, (LATENT, HEADS, VDIM), jnp.float32), -6.0, 6.0) / jnp.sqrt(jnp.float32(LATENT))
    factor = jnp.power(4.0, jnp.arange(HEADS, dtype=jnp.float32) / max(HEADS - 1, 1))
    return (base_draw * factor[None, :, None]).astype(jnp.bfloat16)


def block_levels(rng, extent, split, low, largest):
    def one(axis_at, blocks):
        heights = jax.random.uniform(jax.random.fold_in(jax.random.fold_in(rng, 6), axis_at), (blocks,), jnp.float32, low / len(split), largest / len(split))
        return jnp.repeat(jnp.exp(heights), extent[axis_at] // blocks).reshape((-1,) + (1,) * (len(extent) - axis_at - 1))

    level = one(*split[0])
    for cut in split[1:]:
        level = level * one(*cut)
    return level


def scatter_about(key, shape, scale, reach, split=(), kind=jnp.bfloat16):
    entries = scale * jax.random.normal(key, shape, jnp.float32)
    if split:
        entries = entries * block_levels(key, shape, split, -0.22, 0.18)
    return jnp.clip(entries, -reach, reach).astype(kind)


def setup_inputs(seed: int = 0) -> dict:
    key_list = jax.random.split(jax.random.key(seed), 14)
    stream = scatter_about(key_list[0], (TOKENS, D), 1.0, 6.0, ((0, 128),))
    query_nope = scatter_about(key_list[1], (TOKENS, HEADS, NOPE), 1.0, 6.0, ((0, 16), (1, 8)))
    query_rope = draw_query_rope(jax.random.fold_in(key_list[13], 71), 0)
    latent = scatter_about(key_list[3], (TOKENS, LATENT), 1.0, 6.0, ((0, 16),))
    rope_key = scatter_about(key_list[4], (TOKENS, ROPE), 1.0, 6.0, ((0, 16),))
    latent_gain = jnp.clip(1.0 + 0.18 * jax.random.normal(key_list[5], (LATENT,), jnp.float32), 0.1, 1.9)
    key_up = scatter_about(key_list[6], (LATENT, HEADS, NOPE), (2 * NOPE) ** -0.5, 0.375, ((1, 8),))
    value_up = draw_value_up(jax.random.fold_in(key_list[13], 71), 0)
    out_gain = jnp.clip(1.0 + 0.18 * jax.random.normal(key_list[8], (HEADS * VDIM,), jnp.float32), 0.1, 1.9)
    out_weight = scatter_about(key_list[9], (HEADS * VDIM, D), (HEADS * VDIM) ** -0.5, 0.125, ((0, 8),))
    norm_gain = jnp.clip(1.0 + 0.18 * jax.random.normal(key_list[10], (D,), jnp.float32), 0.1, 1.9)
    ff_in = scatter_about(key_list[11], (D, FF), D ** -0.5, 0.125, ((0, 16), (1, 8)))
    ff_out = scatter_about(key_list[12], (FF, D), FF ** -0.5, 0.0625, ((0, 8), (1, 16)))
    return {"stream": stream, "query_nope": query_nope, "query_rope": query_rope, "latent": latent, "rope_key": rope_key, "latent_gain": latent_gain, "key_up": key_up, "value_up": value_up, "out_gain": out_gain, "out_weight": out_weight, "norm_gain": norm_gain, "ff_in": ff_in, "ff_out": ff_out}


EPS = 1e-06
THETA = 10000.0

def turn(values, positions):
    full_width = values.shape[-1]
    half_width = full_width // 2
    inverse = jnp.power(THETA, -jnp.arange(0, full_width, 2, dtype=jnp.float32) / full_width)
    angles = positions[:, None] * inverse[None, :]
    cosine = jnp.cos(angles)
    sine_part = jnp.sin(angles)
    if values.ndim == 3:
        cosine = cosine[:, None, :]
        sine_part = sine_part[:, None, :]
    vector = values.astype(jnp.float32)
    lower_half = vector[..., :half_width]
    upper_half = vector[..., half_width:]
    return jnp.concatenate([lower_half * cosine - upper_half * sine_part, lower_half * sine_part + upper_half * cosine], axis=-1)

def reference(stream, query_nope, query_rope, latent, rope_key, latent_gain, key_up, value_up, out_gain, out_weight, norm_gain, ff_in, ff_out):
    positions = jnp.arange(TOKENS, dtype=jnp.float32)
    lat_full = latent.astype(jnp.float32)
    normed = (lat_full * lax.rsqrt(lax.optimization_barrier(jnp.mean(lat_full * lat_full, axis=-1, keepdims=True)) + EPS) * latent_gain.astype(jnp.float32)).astype(jnp.bfloat16)
    keys_rot = turn(rope_key, positions).astype(jnp.bfloat16)
    query_rot = turn(query_rope, positions).astype(jnp.bfloat16)
    query_lat = jnp.einsum('thn,lhn->thl', query_nope.astype(jnp.float32), key_up.astype(jnp.float32)).astype(jnp.bfloat16)
    score_scale = 1.0 / math.sqrt(NOPE + ROPE)
    normed_wide = normed.astype(jnp.float32)
    keys_wide = keys_rot.astype(jnp.float32)

    def attend(inputs):
        lat_query, rot_query = inputs
        scores = (jnp.einsum('thl,kl->thk', lat_query.astype(jnp.float32), normed_wide) + jnp.einsum('thr,kr->thk', rot_query.astype(jnp.float32), keys_wide)) * score_scale
        row_max = lax.optimization_barrier(jnp.max(scores, axis=-1, keepdims=True))
        expo = jnp.exp(scores - row_max)
        denom = lax.optimization_barrier(jnp.sum(expo, axis=-1))
        probs = lax.optimization_barrier(expo.astype(jnp.bfloat16)).astype(jnp.float32)
        summed = jnp.einsum('thk,kl->thl', probs, normed_wide)
        return (summed / denom[..., None]).astype(jnp.bfloat16)
    q_block = math.gcd(TOKENS, 512)
    out_lat = lax.map(attend, (query_lat.reshape(TOKENS // q_block, q_block, HEADS, LATENT), query_rot.reshape(TOKENS // q_block, q_block, HEADS, ROPE)))
    out_lat = out_lat.reshape(TOKENS, HEADS, LATENT)
    head_out = jnp.einsum('thl,lhv->thv', out_lat.astype(jnp.float32), value_up.astype(jnp.float32))
    row_scale = lax.rsqrt(lax.optimization_barrier(jnp.mean(head_out * head_out, axis=(1, 2))) + EPS)
    gated = (head_out.reshape(TOKENS, HEADS * VDIM) * out_gain.astype(jnp.float32)).astype(jnp.bfloat16)
    mid_stream = stream.astype(jnp.float32) + row_scale[:, None] * jnp.dot(gated, out_weight, preferred_element_type=jnp.float32)
    ff_input = (mid_stream * lax.rsqrt(lax.optimization_barrier(jnp.mean(mid_stream * mid_stream, axis=-1, keepdims=True)) + EPS) * norm_gain.astype(jnp.float32)).astype(jnp.bfloat16)
    pre_act = jnp.dot(ff_input, ff_in, preferred_element_type=jnp.float32)
    activation = jnp.square(jax.nn.relu(pre_act)).astype(jnp.bfloat16)
    return (mid_stream + jnp.dot(activation, ff_out, preferred_element_type=jnp.float32)).astype(jnp.bfloat16)
```

```python
import functools
import math

import jax
import jax.numpy as jnp
from jax import lax
from jax.experimental import pallas as pl
from jax.experimental.pallas import tpu as pltpu
from jax.sharding import PartitionSpec as P

HEADS = 16
NOPE = 128
ROPE = 64
LATENT = 512
VDIM = 128
RING = 4
SHIFTS = (1, 3, 2)

EPS = 1e-06
THETA = 10000.0
SCALE2 = math.log2(math.e) / math.sqrt(NOPE + ROPE)
LAST_LAST = (((1,), (1,)), ((), ()))


def sp_of(z, y):
    return (z % RING) * RING + (y % RING)


def along_y(values, shift):
    pairs = [(sp_of(z, y), sp_of(z, y + shift)) for z in range(RING) for y in range(RING)]
    return lax.ppermute(values, "sp", pairs)


def along_z(values, shift):
    pairs = [(sp_of(z, y), sp_of(z + shift, y)) for z in range(RING) for y in range(RING)]
    return lax.ppermute(values, "sp", pairs)


def along_x(values, shift):
    pairs = [(2 * x + c, 2 * ((x + shift) % RING) + c) for x in range(RING) for c in range(2)]
    return lax.ppermute(values, "tp", pairs)


def other_core(values):
    return lax.ppermute(values, "tp", [(t, t ^ 1) for t in range(2 * RING)])


def dot32(a, b, dims=None):
    if dims is None:
        return jnp.dot(a, b, preferred_element_type=jnp.float32)
    return lax.dot_general(a, b, dims, preferred_element_type=jnp.float32)


def call(kernel, outs, scratch, flops, moved, name, *args, scalars=0):
    vmem = pl.BlockSpec(memory_space=pltpu.VMEM)
    smem = pl.BlockSpec(memory_space=pltpu.SMEM)
    return pl.pallas_call(
        kernel,
        out_shape=outs,
        in_specs=[smem] * scalars + [vmem] * (len(args) - scalars),
        out_specs=jax.tree.map(lambda _: vmem, outs),
        scratch_shapes=scratch,
        compiler_params=pltpu.CompilerParams(vmem_limit_bytes=40 * 1024 * 1024),
        cost_estimate=pl.CostEstimate(flops=flops, bytes_accessed=moved, transcendentals=0),
        name=name,
    )(*args)


def attend_kernel(q_ref, k_ref, kup_ref, vup_ref, o_ref, qs):
    rows = q_ref.shape[0]
    lane = lax.broadcasted_iota(jnp.int32, (rows, 128), 1)
    rot = q_ref[:, 256:384]
    zero = jnp.zeros_like(rot)
    qs[0:rows, 512:640] = jnp.where(lane < ROPE, rot, zero)
    turned = pltpu.roll(rot.astype(jnp.float32), ROPE, 1).astype(jnp.bfloat16)
    qs[rows : 2 * rows, 512:640] = jnp.where(lane < ROPE, turned, zero)
    for h in range(2):
        qs[h * rows : (h + 1) * rows, 0:512] = dot32(
            q_ref[:, h * 128 : (h + 1) * 128], kup_ref[h], LAST_LAST
        ).astype(jnp.bfloat16)
    stats = jnp.zeros((rows, 128), jnp.float32)
    for h in range(2):
        scores = dot32(qs[h * rows : (h + 1) * rows, :], k_ref[...], LAST_LAST)
        top = jnp.max(scores, axis=1, keepdims=True) * SCALE2
        expo = jnp.exp2(scores * SCALE2 - top)
        total = jnp.sum(expo, axis=1, keepdims=True)
        out = dot32(expo.astype(jnp.bfloat16), k_ref[:, 0:512])
        out = (out / total).astype(jnp.bfloat16)
        o_ref[:, h * 128 : (h + 1) * 128] = dot32(out, vup_ref[h]).astype(jnp.bfloat16)
        lse = top + jnp.log2(total)
        high = lse.astype(jnp.bfloat16).astype(jnp.float32)
        mid = (lse - high).astype(jnp.bfloat16).astype(jnp.float32)
        low = lse - high - mid
        stats = jnp.where(lane == 3 * h, high, stats)
        stats = jnp.where(lane == 3 * h + 1, mid, stats)
        stats = jnp.where(lane == 3 * h + 2, low, stats)
    o_ref[:, 256:384] = stats.astype(jnp.bfloat16)


def attend(queries, keys, kup, vup):
    rows = queries.shape[0]
    count = keys.shape[0]
    return call(
        attend_kernel,
        jax.ShapeDtypeStruct((rows, 384), jnp.bfloat16),
        [pltpu.VMEM((2 * rows, 640), jnp.bfloat16)],
        2 * 2 * rows * count * 1280,
        count * 1280 + rows * 1536,
        "attend",
        queries,
        keys,
        kup,
        vup,
    )


def combine_kernel(a_ref, b_ref, c_ref, d_ref, h_ref):
    rows = a_ref.shape[0]
    lane = lax.broadcasted_iota(jnp.int32, (rows, 128), 1)
    parts = (a_ref, b_ref, c_ref, d_ref)
    stats = [ref[:, 256:384].astype(jnp.float32) for ref in parts]
    for h in range(2):
        mine = (lane >= 3 * h) & (lane < 3 * h + 3)
        lses = [jnp.sum(jnp.where(mine, s, 0.0), axis=1, keepdims=True) for s in stats]
        top = functools.reduce(jnp.maximum, lses)
        shares = [jnp.exp2(v - top) for v in lses]
        whole = shares[0] + shares[1] + shares[2] + shares[3]
        cols = slice(h * 128, (h + 1) * 128)
        summed = sum(s * ref[:, cols].astype(jnp.float32) for s, ref in zip(shares, parts))
        h_ref[:, cols] = (summed / whole).astype(jnp.bfloat16)


def project_kernel(*refs):
    heads, weights, out_ref = refs[0:4], refs[4:8], refs[8]
    rows = heads[0].shape[0]
    for n in range(4):
        cols = slice(n * 512, (n + 1) * 512)
        total = sum(dot32(h[...], w[0:256, cols]) for h, w in zip(heads, weights))
        out_ref[:, cols] = total.astype(jnp.bfloat16)
    squares = sum(
        jnp.sum(jnp.square(h[...].astype(jnp.float32)), axis=1, keepdims=True) for h in heads
    )
    high = squares.astype(jnp.bfloat16).astype(jnp.float32)
    mid = (squares - high).astype(jnp.bfloat16).astype(jnp.float32)
    low = squares - high - mid
    lane = lax.broadcasted_iota(jnp.int32, (rows, 128), 1)
    stats = jnp.where(lane == 0, high, jnp.where(lane == 1, mid, jnp.where(lane == 2, low, 0.0)))
    out_ref[:, 2048:2176] = stats.astype(jnp.bfloat16)


def ff_in_kernel(
    where_ref, own_ref, oth_ref, s0, s1, s2, s3, sb_ref, gain_ref, w0, w1, w2, w3,
    act_ref, mid_ref, xs, xr,
):
    share = mid_ref.shape[0]
    x, c, z, y = where_ref[0], where_ref[1], where_ref[2], where_ref[3]
    gain = gain_ref[...]
    for i in range(8):
        shift = (0, *SHIFTS)[i % 4]
        core = c if i < 4 else 1 - c
        block = lax.rem(x + RING - shift, RING) * 2 + core
        rows = pl.ds(pl.multiple_of(block * share, 16), share)
        both = own_ref[rows, :].astype(jnp.float32) + oth_ref[rows, :].astype(jnp.float32)
        squares = jnp.sum(both[:, 2048:2176], axis=1, keepdims=True)
        scale = lax.rsqrt(squares / (HEADS * VDIM) + EPS)
        if i < 4:
            stream = (s0, s1, s2, s3)[i][256 : 256 + share, :]
        else:
            stream = sb_ref[(i - 4) * share : (i - 3) * share, :]
        mid = stream.astype(jnp.float32) + scale * both[:, 0:2048]
        if i == 0:
            mid_ref[...] = mid
        mean = jnp.mean(mid * mid, axis=1, keepdims=True)
        xs[i * share : (i + 1) * share, :] = (mid * lax.rsqrt(mean + EPS) * gain).astype(jnp.bfloat16)
    order = (0, *SHIFTS)
    for i, dz in enumerate(order):
        for j, dy in enumerate(order):
            block = lax.rem(z + RING - dz, RING) * RING + lax.rem(y + RING - dy, RING)
            cols = pl.ds(pl.multiple_of(block * 128, 128), 128)
            at = (i * 4 + j) * 128
            xr[:, at : at + 128] = xs[:, cols]
    width = act_ref.shape[1]
    for n in range(width // 512):
        cols = slice(n * 512, (n + 1) * 512)
        total = sum(dot32(xr[:, i * 512 : (i + 1) * 512], w[:, cols]) for i, w in enumerate((w0, w1, w2, w3)))
        act_ref[:, cols] = jnp.square(jnp.maximum(total, 0.0)).astype(jnp.bfloat16)


def ff_out_kernel(where_ref, act_ref, w0, w1, w2, w3, keep_ref, send_ref):
    z, y = where_ref[2], where_ref[3]
    half = keep_ref.shape[0]
    order = (0, *SHIFTS)
    for j, dy in enumerate(order):
        w = (w0, w1, w2, w3)[j]
        for pair in range(2):
            both = jnp.concatenate([w[2 * pair], w[2 * pair + 1]], axis=1)
            out = dot32(act_ref[...], both)
            for k in range(2):
                dz = order[2 * pair + k]
                block = lax.rem(z + RING - dz, RING) * RING + lax.rem(y + RING - dy, RING)
                cols = pl.ds(pl.multiple_of(block * 128, 128), 128)
                keep_ref[:, cols] = out[0:half, k * 128 : (k + 1) * 128]
                send_ref[:, cols] = out[half:, k * 128 : (k + 1) * 128].astype(jnp.bfloat16)


def turn(values, positions):
    full_width = values.shape[-1]
    half_width = full_width // 2
    inverse = jnp.power(THETA, -jnp.arange(0, full_width, 2, dtype=jnp.float32) / full_width)
    angles = positions[:, None] * inverse[None, :]
    cosine = jnp.cos(angles)
    sine_part = jnp.sin(angles)
    if values.ndim == 3:
        cosine = cosine[:, None, :]
        sine_part = sine_part[:, None, :]
    vector = values.astype(jnp.float32)
    lower_half = vector[..., :half_width]
    upper_half = vector[..., half_width:]
    return jnp.concatenate(
        [
            lower_half * cosine - upper_half * sine_part,
            lower_half * sine_part + upper_half * cosine,
        ],
        axis=-1,
    )


def body(
    stream,
    query_nope,
    query_rope,
    latent,
    rope_key,
    latent_gain,
    key_up,
    value_up,
    out_gain,
    out_weight,
    norm_gain,
    ff_in,
    ff_out,
):
    bf16 = jnp.bfloat16
    rows = query_nope.shape[0]
    share = stream.shape[0]
    sp, tp = lax.axis_index("sp"), lax.axis_index("tp")
    z, y = sp // RING, sp % RING
    x, core = tp // 2, tp % 2
    where = jnp.stack([x, core, z, y]).astype(jnp.int32)
    positions = (sp * rows + jnp.arange(rows, dtype=jnp.int32)).astype(jnp.float32)

    query_rot = turn(query_rope, positions).astype(bf16)
    queries = jnp.concatenate(
        [query_nope.reshape(rows, 2 * NOPE), query_rot.reshape(rows, 2 * ROPE)], axis=1
    )
    lat_full = latent.astype(jnp.float32)
    normed = (
        lat_full
        * lax.rsqrt(jnp.mean(lat_full * lat_full, axis=-1, keepdims=True) + EPS)
        * latent_gain
    ).astype(bf16)
    keys_rot = turn(rope_key, positions).astype(bf16)
    keys = jnp.concatenate([normed, keys_rot, jnp.zeros((rows, 128 - ROPE), bf16)], axis=1)
    kup = jnp.transpose(key_up, (1, 0, 2))
    vup = jnp.transpose(value_up, (1, 0, 2))

    half_keys = lax.dynamic_slice_in_dim(keys, core * (rows // 2), rows // 2, 0)
    far_queries = [along_y(queries, s) for s in SHIFTS]
    far_keys = jnp.concatenate([along_z(half_keys, s) for s in SHIFTS], axis=0)
    other_keys = other_core(far_keys)
    all_keys = jnp.concatenate([keys, far_keys, other_keys], axis=0)

    scaled_weight = (out_weight.astype(jnp.float32) * out_gain[:, None]).astype(bf16)
    pack = jnp.concatenate([scaled_weight, stream], axis=0)
    packs = [pack] + [along_x(pack, s) for s in SHIFTS]
    other_stream = other_core(jnp.concatenate([p[256:] for p in packs], axis=0))

    in_rows = [ff_in] + [along_y(ff_in, s) for s in SHIFTS]
    out_cols = [ff_out] + [along_z(ff_out, s) for s in SHIFTS]
    in_rows = jnp.concatenate(in_rows, axis=0)
    out_cols = jnp.stack(out_cols, axis=0)
    in_parts = [in_rows] + [along_z(in_rows, s) for s in SHIFTS]
    out_parts = [out_cols] + [along_y(out_cols, s) for s in SHIFTS]

    backs = []
    for s, q in zip(SHIFTS, far_queries):
        backs.append(along_y(attend(q, all_keys, kup, vup), -s))
    mine = attend(queries, all_keys, kup, vup)
    head_out = call(
        combine_kernel,
        jax.ShapeDtypeStruct((rows, 256), bf16),
        [],
        rows * 256 * 16,
        rows * 384 * 2 * 5,
        "combine",
        mine,
        *backs,
    )
    heads = [head_out] + [along_x(head_out, s) for s in SHIFTS]
    projected = call(
        project_kernel,
        jax.ShapeDtypeStruct((rows, 2176), bf16),
        [],
        2 * rows * 1024 * 2048,
        rows * 6400 + 1024 * 4096,
        "project",
        *heads,
        *packs,
    )
    other_projected = other_core(projected)
    activation, mid_stream = call(
        ff_in_kernel,
        (
            jax.ShapeDtypeStruct((rows, ff_in.shape[1]), bf16),
            jax.ShapeDtypeStruct((share, stream.shape[1]), jnp.float32),
        ),
        [pltpu.VMEM((rows, 2048), bf16), pltpu.VMEM((rows, 2048), bf16)],
        2 * rows * 2048 * 1024,
        rows * 10000 + 2048 * 2048,
        "ff_in",
        where,
        projected,
        other_projected,
        *packs,
        other_stream,
        norm_gain[None, :],
        *in_parts,
        scalars=1,
    )
    keep, send = call(
        ff_out_kernel,
        (
            jax.ShapeDtypeStruct((rows // 2, 2048), jnp.float32),
            jax.ShapeDtypeStruct((rows // 2, 2048), bf16),
        ),
        [],
        2 * rows * 2048 * 1024,
        rows * 5000 + 2048 * 2048,
        "ff_out",
        where,
        activation,
        *out_parts,
        scalars=1,
    )
    summed = keep + other_core(send).astype(jnp.float32)
    mixed = summed[0:share]
    for i, s in enumerate(SHIFTS):
        block = summed[(i + 1) * share : (i + 2) * share].astype(bf16)
        mixed = mixed + along_x(block, -s).astype(jnp.float32)
    return (mid_stream + mixed).astype(bf16)


def solution(mesh):
    placed = (
        P(("sp", "tp"), None),
        P("sp", "tp", None),
        P("sp", "tp", None),
        P("sp", None),
        P("sp", None),
        P(),
        P(None, "tp", None),
        P(None, "tp", None),
        P("tp"),
        P("tp", None),
        P(),
        P("sp", "tp"),
        P("tp", "sp"),
    )
    return jax.shard_map(
        body, mesh=mesh, in_specs=placed, out_specs=P(("sp", "tp"), None), check_vma=False
    )
```

```python
import functools
import math

import jax
import jax.numpy as jnp
import numpy as np
from jax import lax
from jax.experimental import pallas as pl
from jax.experimental.pallas import tpu as pltpu
from jax.sharding import PartitionSpec as P


HEADS = 16
NOPE = 128
ROPE = 64
LATENT = 512
VDIM = 128
RING = 4
SHARE = 48
SHIFTS = (1, 3, 2)

EPS = 1e-06
THETA = 10000.0
SCALE2 = math.log2(math.e) / math.sqrt(NOPE + ROPE)
LAST_LAST = (((1,), (1,)), ((), ()))


def sp_of(z, y):
    return (z % RING) * RING + (y % RING)


def along_y(values, shift):
    pairs = [(sp_of(z, y), sp_of(z, y + shift)) for z in range(RING) for y in range(RING)]
    return lax.ppermute(values, "sp", pairs)


def along_z(values, shift):
    pairs = [(sp_of(z, y), sp_of(z + shift, y)) for z in range(RING) for y in range(RING)]
    return lax.ppermute(values, "sp", pairs)


def along_x(values, shift):
    pairs = [(2 * x + c, 2 * ((x + shift) % RING) + c) for x in range(RING) for c in range(2)]
    return lax.ppermute(values, "tp", pairs)


def up_and_down(values):
    pairs = []
    for z in range(RING):
        for y in range(RING):
            for t in range(2 * RING):
                to = sp_of(z + (1 if t % 2 == 0 else -1), y)
                pairs.append((sp_of(z, y) * 2 * RING + t, to * 2 * RING + t))
    return lax.ppermute(values, ("sp", "tp"), pairs)


def other_core(values):
    return lax.ppermute(values, "tp", [(t, t ^ 1) for t in range(2 * RING)])


def dot32(a, b, dims=None):
    if dims is None:
        return jnp.dot(a, b, preferred_element_type=jnp.float32)
    return lax.dot_general(a, b, dims, preferred_element_type=jnp.float32)


def call(kernel, outs, scratch, flops, moved, *args, scalars=0, remote=()):
    vmem = pl.BlockSpec(memory_space=pltpu.VMEM)
    smem = pl.BlockSpec(memory_space=pltpu.SMEM)
    hbm = pl.BlockSpec(memory_space=pltpu.HBM)
    return pl.pallas_call(
        kernel,
        out_shape=outs,
        in_specs=[smem if i < scalars else hbm if i in remote else vmem for i in range(len(args))],
        out_specs=jax.tree.map(lambda _: vmem, outs),
        scratch_shapes=scratch,
        compiler_params=pltpu.CompilerParams(vmem_limit_bytes=40 * 1024 * 1024),
        cost_estimate=pl.CostEstimate(flops=flops, bytes_accessed=moved, transcendentals=0),
    )(*args)


def join_kernel(a_ref, b_ref, c_ref, d_ref, o_ref):
    for i, ref in enumerate((a_ref, b_ref, c_ref, d_ref)):
        o_ref[i] = ref[...]


def join(parts):
    shape = parts[0].shape
    moved = 16 * shape[0] * shape[1]
    return call(join_kernel, jax.ShapeDtypeStruct((4, *shape), parts[0].dtype), [], moved, moved, *parts)


def fetch(sources, targets, sems):
    copies = [pltpu.make_async_copy(s, t, sems.at[i]) for i, (s, t) in enumerate(zip(sources, targets))]
    for c in copies:
        c.start()
    return copies


def angles(inverse, start, rows):
    token = (start + lax.broadcasted_iota(jnp.int32, (1, rows), 1)).astype(jnp.float32)
    angle = inverse * token
    return jnp.cos(angle), jnp.sin(angle)


def rotated(ref, at, cosine, sine):
    pairs = ROPE // 2
    low = ref[at : at + pairs, :].astype(jnp.float32)
    high = ref[at + pairs : at + ROPE, :].astype(jnp.float32)
    return [low * cosine - high * sine, low * sine + high * cosine]


def keys_kernel(
    where_ref, latent_hbm, key_hbm, gain_hbm, inverse_hbm, k_ref, half_ref, cos_ref, sin_ref,
    latent_ref, key_ref, gain_ref, inverse_ref, sems,
):
    rows = k_ref.shape[0]
    half = rows // 2
    sources = (inverse_hbm, key_hbm, gain_hbm, latent_hbm)
    copies = fetch(sources, (inverse_ref, key_ref, gain_ref, latent_ref), sems)
    copies[0].wait()
    cosine, sine = angles(inverse_ref[...], where_ref[4], rows)
    cos_ref[...] = cosine
    sin_ref[...] = sine
    copies[1].wait()
    zeros = jnp.zeros((ROPE, rows), jnp.float32)
    keys = jnp.concatenate(rotated(key_ref, 0, cosine, sine) + [zeros], axis=0)
    k_ref[:, LATENT : LATENT + 128] = jnp.transpose(keys).astype(jnp.bfloat16)
    copies[2].wait()
    copies[3].wait()
    lat = latent_ref[...].astype(jnp.float32)
    mean = jnp.mean(lat * lat, axis=1, keepdims=True)
    k_ref[:, 0:LATENT] = (lat * lax.rsqrt(mean + EPS) * gain_ref[...]).astype(jnp.bfloat16)
    half_ref[...] = k_ref[pl.ds(pl.multiple_of(where_ref[1] * half, 64), half), :]


def queries_kernel(nope_ref, rope_ref, cos_ref, sin_ref, q_ref):
    cosine, sine = cos_ref[...], sin_ref[...]
    parts = rotated(rope_ref, 0, cosine, sine) + rotated(rope_ref, ROPE, cosine, sine)
    q_ref[:, 0:256] = nope_ref[...]
    q_ref[:, 256:384] = jnp.transpose(jnp.concatenate(parts, axis=0)).astype(jnp.bfloat16)


def attend_kernel(q_ref, k_ref, kup_ref, vup_ref, o_ref, qs):
    rows = q_ref.shape[0]
    lane = lax.broadcasted_iota(jnp.int32, (rows, 128), 1)

    def head(h, stats):
        cols = pl.ds(pl.multiple_of(h * 128, 128), 128)
        rot = q_ref[:, 256:384].astype(jnp.float32)
        rot = jnp.where(h == 0, rot, pltpu.roll(rot, ROPE, 1))
        qs[:, 512:640] = jnp.where(lane < ROPE, rot, 0.0).astype(jnp.bfloat16)
        qs[:, 0:512] = dot32(q_ref[:, cols], kup_ref[h], LAST_LAST).astype(jnp.bfloat16)
        scores = dot32(qs[...], k_ref[...], LAST_LAST)
        top = jnp.max(scores, axis=1, keepdims=True) * SCALE2
        expo = jnp.exp2(scores * SCALE2 - top)
        total = jnp.sum(expo, axis=1, keepdims=True)
        out = dot32(expo.astype(jnp.bfloat16), k_ref[:, 0:512])
        out = (out / total).astype(jnp.bfloat16)
        o_ref[:, cols] = dot32(out, vup_ref[h]).astype(jnp.bfloat16)
        lse = top + jnp.log2(total)
        high = lse.astype(jnp.bfloat16).astype(jnp.float32)
        mid = (lse - high).astype(jnp.bfloat16).astype(jnp.float32)
        low = lse - high - mid
        stats = jnp.where(lane == 3 * h, high, stats)
        stats = jnp.where(lane == 3 * h + 1, mid, stats)
        return jnp.where(lane == 3 * h + 2, low, stats)

    stats = lax.fori_loop(0, 2, head, jnp.zeros((rows, 128), jnp.float32))
    o_ref[:, 256:384] = stats.astype(jnp.bfloat16)


def attend(queries, keys, kup, vup):
    rows = queries.shape[0]
    count = keys.shape[0]
    return call(
        attend_kernel,
        jax.ShapeDtypeStruct((rows, 384), jnp.bfloat16),
        [pltpu.VMEM((rows, 640), jnp.bfloat16)],
        2 * 2 * rows * count * 1280,
        count * 1280 + rows * 1536,
        queries,
        keys,
        kup,
        vup,
    )


def combine_kernel(a_ref, b_ref, c_ref, d_ref, h_ref):
    rows = a_ref.shape[0]
    lane = lax.broadcasted_iota(jnp.int32, (rows, 128), 1)
    parts = (a_ref, b_ref, c_ref, d_ref)
    stats = [ref[:, 256:384].astype(jnp.float32) for ref in parts]
    for h in range(2):
        mine = (lane >= 3 * h) & (lane < 3 * h + 3)
        lses = [jnp.sum(jnp.where(mine, s, 0.0), axis=1, keepdims=True) for s in stats]
        top = functools.reduce(jnp.maximum, lses)
        shares = [jnp.exp2(v - top) for v in lses]
        whole = shares[0] + shares[1] + shares[2] + shares[3]
        cols = slice(h * 128, (h + 1) * 128)
        summed = sum(s * ref[:, cols].astype(jnp.float32) for s, ref in zip(shares, parts))
        h_ref[:, cols] = (summed / whole).astype(jnp.bfloat16)


def project_kernel(h0, h1, h2, h3, w0, w1, w2, w3a, w3b, out_ref):
    heads = (h0, h1, h2, h3)
    rows = h0.shape[0]
    for n in range(4):
        cols = slice(n * 512, (n + 1) * 512)
        total = sum(dot32(h[...], w[SHARE : SHARE + 256, cols]) for h, w in zip(heads, (w0, w1, w2)))
        last = jnp.concatenate([w3a[SHARE : SHARE + 128, cols], w3b[:, cols]], axis=0)
        out_ref[:, cols] = (total + dot32(h3[...], last)).astype(jnp.bfloat16)
    squares = sum(
        jnp.sum(jnp.square(h[...].astype(jnp.float32)), axis=1, keepdims=True) for h in heads
    )
    high = squares.astype(jnp.bfloat16).astype(jnp.float32)
    mid = (squares - high).astype(jnp.bfloat16).astype(jnp.float32)
    low = squares - high - mid
    lane = lax.broadcasted_iota(jnp.int32, (rows, 128), 1)
    stats = jnp.where(lane == 0, high, jnp.where(lane == 1, mid, jnp.where(lane == 2, low, 0.0)))
    out_ref[:, 2048:2176] = stats.astype(jnp.bfloat16)


def ff_in_kernel(
    where_ref, own_ref, oth_ref, sa_ref, sb_ref, gain_ref, w0, w1, w2, w3a, w3b,
    act_ref, mid_ref, xs, xr,
):
    share = mid_ref.shape[0]
    x, c, z, y = where_ref[0], where_ref[1], where_ref[2], where_ref[3]
    gain = gain_ref[...]
    for i in range(8):
        shift = (0, *SHIFTS)[i % 4]
        core = c if i < 4 else 1 - c
        block = lax.rem(x + RING - shift, RING) * 2 + core
        rows = pl.ds(pl.multiple_of(block * share, 16), share)
        both = own_ref[rows, :].astype(jnp.float32) + oth_ref[rows, :].astype(jnp.float32)
        squares = jnp.sum(both[:, 2048:2176], axis=1, keepdims=True)
        scale = lax.rsqrt(squares / (HEADS * VDIM) + EPS)
        at = (i % 4) * share
        stream = (sa_ref if i < 4 else sb_ref)[at : at + share, :]
        mid = stream.astype(jnp.float32) + scale * both[:, 0:2048]
        if i == 0:
            mid_ref[...] = mid
        mean = jnp.mean(mid * mid, axis=1, keepdims=True)
        xs[i * share : (i + 1) * share, :] = (mid * lax.rsqrt(mean + EPS) * gain).astype(jnp.bfloat16)
    order = (0, *SHIFTS)
    for i, dz in enumerate(order):
        for j, dy in enumerate(order):
            block = lax.rem(z + RING - dz, RING) * RING + lax.rem(y + RING - dy, RING)
            cols = pl.ds(pl.multiple_of(block * 128, 128), 128)
            at = (i * 4 + j) * 128
            xr[:, at : at + 128] = xs[:, cols]
    width = act_ref.shape[1]
    for n in range(width // 512):
        cols = slice(n * 512, (n + 1) * 512)
        total = jnp.zeros((xr.shape[0], 512), jnp.float32)
        for i, w in enumerate((w0, w1, w2)):
            piece = jnp.concatenate([w[k, :, cols] for k in range(4)], axis=0)
            total += dot32(xr[:, i * 512 : (i + 1) * 512], piece)
        piece = jnp.concatenate([w[k, :, cols] for w in (w3a, w3b) for k in range(2)], axis=0)
        total += dot32(xr[:, 1536:2048], piece)
        act_ref[:, cols] = jnp.square(jnp.maximum(total, 0.0)).astype(jnp.bfloat16)


def ff_out_kernel(act_ref, *refs):
    pieces, keep_ref, send_ref = refs[:-2], refs[-2], refs[-1]
    half = keep_ref.shape[0]
    at = 0
    for w in pieces:
        for pair in range(w.shape[0] // 2):
            both = jnp.concatenate([w[2 * pair], w[2 * pair + 1]], axis=1)
            out = dot32(act_ref[...], both)
            keep_ref[:, at : at + 256] = out[0:half]
            send_ref[:, at : at + 256] = out[half:].astype(jnp.bfloat16)
            at += 256


def second_layer(activation, *pieces):
    rows, hidden = activation.shape
    width = 128 * sum(p.shape[0] for p in pieces)
    outs = (
        jax.ShapeDtypeStruct((rows // 2, width), jnp.float32),
        jax.ShapeDtypeStruct((rows // 2, width), jnp.bfloat16),
    )
    flops = 2 * rows * hidden * width
    return call(ff_out_kernel, outs, [], flops, 4 * hidden * width, activation, *pieces)


def finish_kernel(where_ref, mid_ref, keep_a, a1, a2, a3, keep_b, b1, b2, b3, out_ref):
    z, y = where_ref[2], where_ref[3]
    share = mid_ref.shape[0]
    at = 0
    for dy, keep, others in (
        (0, keep_a, (a1, a2, a3)),
        (1, keep_a, (a1, a2, a3)),
        (3, keep_a, (a1, a2, a3)),
        (2, keep_b, (b1, b2, b3)),
    ):
        at = 0 if dy == 2 else at
        for dz in (0, *SHIFTS):
            block = lax.rem(z + RING - dz, RING) * RING + lax.rem(y + RING - dy, RING)
            cols = pl.ds(pl.multiple_of(block * 128, 128), 128)
            total = mid_ref[:, cols] + keep[0:share, at : at + 128]
            for other in others:
                total += other[:, at : at + 128].astype(jnp.float32)
            out_ref[:, cols] = total.astype(jnp.bfloat16)
            at += 128


def body(
    stream,
    query_nope,
    query_rope,
    latent,
    rope_key,
    latent_gain,
    key_up,
    value_up,
    out_gain,
    out_weight,
    norm_gain,
    ff_in,
    ff_out,
):
    bf16 = jnp.bfloat16
    rows = query_nope.shape[0]
    share = stream.shape[0]
    sp, tp = lax.axis_index("sp"), lax.axis_index("tp")
    where = jnp.stack([tp // 2, tp % 2, sp // RING, sp % RING, sp * rows]).astype(jnp.int32)

    inverse = np.power(np.float32(THETA), -np.arange(0, ROPE, 2, dtype=np.float32) / ROPE)
    keys, half_keys, cosine, sine = call(
        keys_kernel,
        (
            jax.ShapeDtypeStruct((rows, 640), bf16),
            jax.ShapeDtypeStruct((rows // 2, 640), bf16),
            jax.ShapeDtypeStruct((ROPE // 2, rows), jnp.float32),
            jax.ShapeDtypeStruct((ROPE // 2, rows), jnp.float32),
        ),
        [
            pltpu.VMEM((rows, LATENT), bf16),
            pltpu.VMEM((ROPE, rows), bf16),
            pltpu.VMEM((1, LATENT), jnp.float32),
            pltpu.VMEM((ROPE // 2, 1), jnp.float32),
            pltpu.SemaphoreType.DMA((4,)),
        ],
        rows * 2048,
        rows * 2048,
        where,
        latent,
        jnp.transpose(rope_key),
        latent_gain[None, :],
        inverse[:, None],
        scalars=1,
        remote=(1, 2, 3, 4),
    )
    queries = call(
        queries_kernel,
        jax.ShapeDtypeStruct((rows, 384), bf16),
        [],
        rows * 2048,
        rows * 2048,
        query_nope.reshape(rows, 2 * NOPE),
        jnp.transpose(query_rope, (1, 2, 0)).reshape(2 * ROPE, rows),
        cosine,
        sine,
    )
    kup = jnp.transpose(key_up, (1, 0, 2))
    vup = jnp.transpose(value_up, (1, 0, 2))
    near_keys = up_and_down(keys)
    far_keys = jnp.concatenate([near_keys, along_z(half_keys, 2)], axis=0)
    other_keys = other_core(far_keys)
    all_keys = jnp.concatenate([keys, far_keys, other_keys], axis=0)
    far_queries = [along_y(queries, s) for s in SHIFTS]

    scaled_weight = (out_weight.astype(jnp.float32) * out_gain[:, None]).astype(bf16)
    pack = jnp.concatenate([stream, scaled_weight], axis=0)
    cut = share + 128
    pack1, pack3 = along_x(pack, 1), along_x(pack, 3)
    pack2a = along_x(pack1[:cut], 1)
    pack2b = along_x(pack3[cut:], 3)
    own_stream = jnp.concatenate([p[:share] for p in (pack, pack1, pack3, pack2a)], axis=0)
    other_stream = other_core(own_stream)

    in_rows = join([ff_in] + [along_y(ff_in, s) for s in SHIFTS])
    out_cols = join([ff_out] + [along_z(ff_out, s) for s in SHIFTS])
    in1, in3 = along_z(in_rows, 1), along_z(in_rows, 3)
    in2a, in2b = along_z(in1[:2], 1), along_z(in3[2:], 3)
    out1, out3 = along_y(out_cols, 1), along_y(out_cols, 3)
    out2a, out2b = along_y(out1[:2], 1), along_y(out3[2:], 3)

    backs = []
    for s, q in zip(SHIFTS, far_queries):
        backs.append(along_y(attend(q, all_keys, kup, vup), -s))
    mine = attend(queries, all_keys, kup, vup)
    head_out = call(
        combine_kernel,
        jax.ShapeDtypeStruct((rows, 256), bf16),
        [],
        rows * 256 * 16,
        rows * 384 * 2 * 5,
        mine,
        *backs,
    )
    heads = [head_out] + [along_x(head_out, s) for s in SHIFTS]
    projected = call(
        project_kernel,
        jax.ShapeDtypeStruct((rows, 2176), bf16),
        [],
        2 * rows * 1024 * 2048,
        rows * 6400 + 1024 * 4096,
        *heads,
        pack,
        pack1,
        pack3,
        pack2a,
        pack2b,
    )
    other_projected = other_core(projected)
    activation, mid_stream = call(
        ff_in_kernel,
        (
            jax.ShapeDtypeStruct((rows, ff_in.shape[1]), bf16),
            jax.ShapeDtypeStruct((share, stream.shape[1]), jnp.float32),
        ),
        [pltpu.VMEM((rows, 2048), bf16), pltpu.VMEM((rows, 2048), bf16)],
        2 * rows * 2048 * 1024,
        rows * 10000 + 2048 * 2048,
        where,
        projected,
        other_projected,
        own_stream,
        other_stream,
        norm_gain[None, :],
        in_rows,
        in1,
        in3,
        in2a,
        in2b,
        scalars=1,
    )

    def reduced(*pieces):
        keep, send = second_layer(activation, *pieces)
        summed = keep + other_core(send).astype(jnp.float32)
        arrived = []
        for i, s in enumerate(SHIFTS):
            block = summed[(i + 1) * share : (i + 2) * share].astype(bf16)
            arrived.append(along_x(block, -s))
        return summed[0:share], *arrived

    first = reduced(out_cols, out1, out3)
    last = reduced(out2a, out2b)
    return call(
        finish_kernel,
        jax.ShapeDtypeStruct((share, stream.shape[1]), bf16),
        [],
        share * 2048 * 8,
        share * 2048 * 16,
        where,
        mid_stream,
        *first,
        *last,
        scalars=1,
    )


def solution(mesh):
    placed = (
        P(("sp", "tp"), None),
        P("sp", "tp", None),
        P("sp", "tp", None),
        P("sp", None),
        P("sp", None),
        P(),
        P(None, "tp", None),
        P(None, "tp", None),
        P("tp"),
        P("tp", None),
        P(),
        P("sp", "tp"),
        P("tp", "sp"),
    )

    return jax.shard_map(
        body, mesh=mesh, in_specs=placed, out_specs=P(("sp", "tp"), None), check_vma=False
    )
```

```python
import functools
import math

import jax
import jax.numpy as jnp
import numpy as np
from jax import lax
from jax.experimental import pallas as pl
from jax.experimental.pallas import tpu as pltpu
from jax.sharding import PartitionSpec as P


HEADS = 16
NOPE = 128
ROPE = 64
LATENT = 512
VDIM = 128
RING = 4
SHARE = 48
SHIFTS = (1, 3, 2)

EPS = 1e-06
THETA = 10000.0
SCALE2 = math.log2(math.e) / math.sqrt(NOPE + ROPE)
LAST_LAST = (((1,), (1,)), ((), ()))


def sp_of(z, y):
    return (z % RING) * RING + (y % RING)


def along(line, values, shift):
    pairs = []
    for z in range(RING):
        for y in range(RING):
            for t in range(2 * RING):
                on_y = (line == "a") == (t % 2 == 0)
                to = sp_of(z, y + shift) if on_y else sp_of(z + shift, y)
                pairs.append((sp_of(z, y) * 2 * RING + t, to * 2 * RING + t))
    return lax.ppermute(values, ("sp", "tp"), pairs)


def along_x(values, shift):
    pairs = [(2 * x + c, 2 * ((x + shift) % RING) + c) for x in range(RING) for c in range(2)]
    return lax.ppermute(values, "tp", pairs)


def other_core(values):
    return lax.ppermute(values, "tp", [(t, t ^ 1) for t in range(2 * RING)])


def dot32(a, b, dims=None):
    if dims is None:
        return jnp.dot(a, b, preferred_element_type=jnp.float32)
    return lax.dot_general(a, b, dims, preferred_element_type=jnp.float32)


def call(kernel, outs, scratch, flops, moved, *args, scalars=0):
    vmem = pl.BlockSpec(memory_space=pltpu.VMEM)
    smem = pl.BlockSpec(memory_space=pltpu.SMEM)
    return pl.pallas_call(
        kernel,
        out_shape=outs,
        in_specs=[smem] * scalars + [vmem] * (len(args) - scalars),
        out_specs=jax.tree.map(lambda _: vmem, outs),
        scratch_shapes=scratch,
        compiler_params=pltpu.CompilerParams(vmem_limit_bytes=24 * 1024 * 1024),
        cost_estimate=pl.CostEstimate(flops=flops, bytes_accessed=moved, transcendentals=0),
    )(*args)


def join_kernel(a_ref, b_ref, c_ref, d_ref, o_ref):
    for i, ref in enumerate((a_ref, b_ref, c_ref, d_ref)):
        o_ref[i] = ref[...]


def join(parts):
    shape = parts[0].shape
    moved = 16 * shape[0] * shape[1]
    return call(join_kernel, jax.ShapeDtypeStruct((4, *shape), parts[0].dtype), [], moved, moved, *parts)


def angles(start, rows):
    values = np.power(np.float32(THETA), -np.arange(0, ROPE, 2, dtype=np.float32) / ROPE)
    index = lax.broadcasted_iota(jnp.int32, (ROPE // 2, 1), 0)
    inverse = jnp.zeros((ROPE // 2, 1), jnp.float32)
    for i, value in enumerate(values):
        inverse = jnp.where(index == i, float(value), inverse)
    token = (start + lax.broadcasted_iota(jnp.int32, (1, rows), 1)).astype(jnp.float32)
    angle = inverse * token
    return jnp.cos(angle), jnp.sin(angle)


def rotated(ref, at, cosine, sine):
    pairs = ROPE // 2
    low = ref[at : at + pairs, :].astype(jnp.float32)
    high = ref[at + pairs : at + ROPE, :].astype(jnp.float32)
    return [low * cosine - high * sine, low * sine + high * cosine]


def keys_kernel(where_ref, latent_ref, key_ref, gain_ref, k_ref, cos_ref, sin_ref):
    rows = k_ref.shape[0]
    cosine, sine = angles(where_ref[4], rows)
    cos_ref[...] = cosine
    sin_ref[...] = sine
    zeros = jnp.zeros((ROPE, rows), jnp.float32)
    keys = jnp.concatenate(rotated(key_ref, 0, cosine, sine) + [zeros], axis=0)
    k_ref[:, LATENT : LATENT + 128] = jnp.transpose(keys).astype(jnp.bfloat16)
    lat = latent_ref[...].astype(jnp.float32)
    mean = jnp.mean(lat * lat, axis=1, keepdims=True)
    k_ref[:, 0:LATENT] = (lat * lax.rsqrt(mean + EPS) * gain_ref[...]).astype(jnp.bfloat16)


def pack_kernel(in_ref, out_ref, pack_ref):
    hidden = out_ref.shape[0]
    pack_ref[0:hidden, :] = out_ref[...]
    for n in range(hidden // 128):
        pack_ref[hidden + n * 128 : hidden + (n + 1) * 128, :] = in_ref[:, n * 128 : (n + 1) * 128]


def queries_kernel(nope_ref, rope_ref, cos_ref, sin_ref, q_ref):
    cosine, sine = cos_ref[...], sin_ref[...]
    parts = rotated(rope_ref, 0, cosine, sine) + rotated(rope_ref, ROPE, cosine, sine)
    q_ref[:, 0:256] = nope_ref[...]
    q_ref[:, 256:384] = jnp.transpose(jnp.concatenate(parts, axis=0)).astype(jnp.bfloat16)


def attend_kernel(q_ref, k_ref, kup_ref, vup_ref, o_ref, qs):
    rows = q_ref.shape[0]
    lane = lax.broadcasted_iota(jnp.int32, (rows, 128), 1)

    def head(h, stats):
        cols = pl.ds(pl.multiple_of(h * 128, 128), 128)
        rot = q_ref[:, 256:384].astype(jnp.float32)
        rot = jnp.where(h == 0, rot, pltpu.roll(rot, ROPE, 1))
        qs[:, 512:640] = jnp.where(lane < ROPE, rot, 0.0).astype(jnp.bfloat16)
        qs[:, 0:512] = dot32(q_ref[:, cols], kup_ref[h], LAST_LAST).astype(jnp.bfloat16)
        scores = dot32(qs[...], k_ref[...], LAST_LAST)
        top = jnp.max(scores, axis=1, keepdims=True) * SCALE2
        expo = jnp.exp2(scores * SCALE2 - top)
        total = jnp.sum(expo, axis=1, keepdims=True)
        out = dot32(expo.astype(jnp.bfloat16), k_ref[:, 0:512])
        out = (out / total).astype(jnp.bfloat16)
        o_ref[:, cols] = dot32(out, vup_ref[h]).astype(jnp.bfloat16)
        lse = top + jnp.log2(total)
        high = lse.astype(jnp.bfloat16).astype(jnp.float32)
        mid = (lse - high).astype(jnp.bfloat16).astype(jnp.float32)
        low = lse - high - mid
        stats = jnp.where(lane == 3 * h, high, stats)
        stats = jnp.where(lane == 3 * h + 1, mid, stats)
        return jnp.where(lane == 3 * h + 2, low, stats)

    stats = lax.fori_loop(0, 2, head, jnp.zeros((rows, 128), jnp.float32))
    o_ref[:, 256:384] = stats.astype(jnp.bfloat16)


def attend(queries, keys, kup, vup):
    rows = queries.shape[0]
    count = keys.shape[0]
    return call(
        attend_kernel,
        jax.ShapeDtypeStruct((rows, 384), jnp.bfloat16),
        [pltpu.VMEM((rows, 640), jnp.bfloat16)],
        2 * 2 * rows * count * 1280,
        count * 1280 + rows * 1536,
        queries,
        keys,
        kup,
        vup,
    )


def combine_kernel(a_ref, b_ref, c_ref, d_ref, h_ref):
    rows = a_ref.shape[0]
    lane = lax.broadcasted_iota(jnp.int32, (rows, 128), 1)
    parts = (a_ref, b_ref, c_ref, d_ref)
    stats = [ref[:, 256:384].astype(jnp.float32) for ref in parts]
    for h in range(2):
        mine = (lane >= 3 * h) & (lane < 3 * h + 3)
        lses = [jnp.sum(jnp.where(mine, s, 0.0), axis=1, keepdims=True) for s in stats]
        top = functools.reduce(jnp.maximum, lses)
        shares = [jnp.exp2(v - top) for v in lses]
        whole = shares[0] + shares[1] + shares[2] + shares[3]
        cols = slice(h * 128, (h + 1) * 128)
        summed = sum(s * ref[:, cols].astype(jnp.float32) for s, ref in zip(shares, parts))
        h_ref[:, cols] = (summed / whole).astype(jnp.bfloat16)


def project_kernel(h0, h1, h2, h3, w0, w1, w2, w3a, w3b, out_ref):
    heads = (h0, h1, h2, h3)
    rows = h0.shape[0]
    for n in range(4):
        cols = slice(n * 512, (n + 1) * 512)
        total = sum(dot32(h[...], w[SHARE : SHARE + 256, cols]) for h, w in zip(heads, (w0, w1, w2)))
        last = jnp.concatenate([w3a[SHARE : SHARE + 128, cols], w3b[:, cols]], axis=0)
        out_ref[:, cols] = (total + dot32(h3[...], last)).astype(jnp.bfloat16)
    squares = sum(
        jnp.sum(jnp.square(h[...].astype(jnp.float32)), axis=1, keepdims=True) for h in heads
    )
    high = squares.astype(jnp.bfloat16).astype(jnp.float32)
    mid = (squares - high).astype(jnp.bfloat16).astype(jnp.float32)
    low = squares - high - mid
    lane = lax.broadcasted_iota(jnp.int32, (rows, 128), 1)
    stats = jnp.where(lane == 0, high, jnp.where(lane == 1, mid, jnp.where(lane == 2, low, 0.0)))
    out_ref[:, 2048:2176] = stats.astype(jnp.bfloat16)


def ff_in_kernel(
    where_ref, own_ref, oth_ref, sa_ref, sb_ref, gain_ref, w0, w1, w2, w3a, w3b,
    act_ref, mid_ref, xs, xr,
):
    share = mid_ref.shape[0]
    x, c = where_ref[0], where_ref[1]
    gain = gain_ref[...]
    for i in range(8):
        shift = (0, *SHIFTS)[i % 4]
        core = c if i < 4 else 1 - c
        block = lax.rem(x + RING - shift, RING) * 2 + core
        rows = pl.ds(pl.multiple_of(block * share, 16), share)
        both = own_ref[rows, :].astype(jnp.float32) + oth_ref[rows, :].astype(jnp.float32)
        squares = jnp.sum(both[:, 2048:2176], axis=1, keepdims=True)
        scale = lax.rsqrt(squares / (HEADS * VDIM) + EPS)
        at = (i % 4) * share
        stream = (sa_ref if i < 4 else sb_ref)[at : at + share, :]
        mid = stream.astype(jnp.float32) + scale * both[:, 0:2048]
        if i == 0:
            mid_ref[...] = mid
        mean = jnp.mean(mid * mid, axis=1, keepdims=True)
        xs[i * share : (i + 1) * share, :] = (mid * lax.rsqrt(mean + EPS) * gain).astype(jnp.bfloat16)
    for i, block in enumerate(blocks_of(where_ref)):
        cols = pl.ds(pl.multiple_of(block * 128, 128), 128)
        xr[:, i * 128 : (i + 1) * 128] = xs[:, cols]
    hidden = act_ref.shape[1]
    pieces = [(w, k) for w in (w0, w1, w2, w3a, w3b) for k in range(w.shape[0])]
    for n in range(0, hidden // 128, 2):
        columns = []
        for m in (n, n + 1):
            at = hidden + m * 128
            columns.append(jnp.concatenate([w[k, at : at + 128, :] for w, k in pieces], axis=0))
        total = dot32(xr[...], jnp.concatenate(columns, axis=1))
        act_ref[:, n * 128 : (n + 2) * 128] = jnp.square(jnp.maximum(total, 0.0)).astype(jnp.bfloat16)


def blocks_of(where_ref):
    core, z, y = where_ref[1], where_ref[2], where_ref[3]
    order = (0, *SHIFTS)
    blocks = []
    for outer in order:
        for inner in order:
            dz = jnp.where(core == 0, outer, inner)
            dy = jnp.where(core == 0, inner, outer)
            blocks.append(lax.rem(z + RING - dz, RING) * RING + lax.rem(y + RING - dy, RING))
    return blocks


def ff_out_kernel(where_ref, act_ref, w0, w1, w2, w3a, w3b, keep_ref, send_ref):
    half = keep_ref.shape[0]
    hidden = act_ref.shape[1]
    blocks = blocks_of(where_ref)
    pieces = [(w, k) for w in (w0, w1, w2, w3a, w3b) for k in range(w.shape[0])]
    for i in range(0, len(pieces), 2):
        both = jnp.concatenate([w[k, 0:hidden, :] for w, k in pieces[i : i + 2]], axis=1)
        out = dot32(act_ref[...], both)
        for k in range(2):
            cols = pl.ds(pl.multiple_of(blocks[i + k] * 128, 128), 128)
            keep_ref[:, cols] = out[0:half, k * 128 : (k + 1) * 128]
            send_ref[:, cols] = out[half:, k * 128 : (k + 1) * 128].astype(jnp.bfloat16)


def body(
    stream,
    query_nope,
    query_rope,
    latent,
    rope_key,
    latent_gain,
    key_up,
    value_up,
    out_gain,
    out_weight,
    norm_gain,
    ff_in,
    ff_out,
):
    bf16 = jnp.bfloat16
    rows = query_nope.shape[0]
    share = stream.shape[0]
    sp, tp = lax.axis_index("sp"), lax.axis_index("tp")
    where = jnp.stack([tp // 2, tp % 2, sp // RING, sp % RING, sp * rows]).astype(jnp.int32)

    keys, cosine, sine = call(
        keys_kernel,
        (
            jax.ShapeDtypeStruct((rows, 640), bf16),
            jax.ShapeDtypeStruct((ROPE // 2, rows), jnp.float32),
            jax.ShapeDtypeStruct((ROPE // 2, rows), jnp.float32),
        ),
        [],
        rows * 2048,
        rows * 2048,
        where,
        latent,
        jnp.transpose(rope_key),
        latent_gain[None, :],
        scalars=1,
    )
    queries = call(
        queries_kernel,
        jax.ShapeDtypeStruct((rows, 384), bf16),
        [],
        rows * 2048,
        rows * 2048,
        query_nope.reshape(rows, 2 * NOPE),
        jnp.transpose(query_rope, (1, 2, 0)).reshape(2 * ROPE, rows),
        cosine,
        sine,
    )
    kup = jnp.transpose(key_up, (1, 0, 2))
    vup = jnp.transpose(value_up, (1, 0, 2))
    all_keys = jnp.concatenate([keys] + [along("b", keys, s) for s in SHIFTS], axis=0)
    far_queries = [along("a", queries, s) for s in SHIFTS]

    scaled_weight = (out_weight.astype(jnp.float32) * out_gain[:, None]).astype(bf16)
    pack = jnp.concatenate([stream, scaled_weight], axis=0)
    cut = share + 128
    pack1, pack3 = along_x(pack, 1), along_x(pack, 3)
    pack2a = along_x(pack1[:cut], 1)
    pack2b = along_x(pack3[cut:], 3)
    own_stream = jnp.concatenate([p[:share] for p in (pack, pack1, pack3, pack2a)], axis=0)
    other_stream = other_core(own_stream)

    hidden = ff_in.shape[1]
    weights = call(
        pack_kernel,
        jax.ShapeDtypeStruct((2 * hidden, 128), bf16),
        [],
        hidden * 128,
        hidden * 1024,
        ff_in,
        ff_out,
    )
    line = join([weights] + [along("a", weights, s) for s in SHIFTS])
    line1, line3 = along("b", line, 1), along("b", line, 3)
    line2a, line2b = along("b", line1[:2], 1), along("b", line3[2:], 3)
    lines = (line, line1, line3, line2a, line2b)

    backs = []
    for s, q in zip(SHIFTS, far_queries):
        backs.append(along("a", attend(q, all_keys, kup, vup), -s))
    mine = attend(queries, all_keys, kup, vup)
    head_out = call(
        combine_kernel,
        jax.ShapeDtypeStruct((rows, 256), bf16),
        [],
        rows * 256 * 16,
        rows * 384 * 2 * 5,
        mine,
        *backs,
    )
    heads = [head_out] + [along_x(head_out, s) for s in SHIFTS]
    projected = call(
        project_kernel,
        jax.ShapeDtypeStruct((rows, 2176), bf16),
        [],
        2 * rows * 1024 * 2048,
        rows * 6400 + 1024 * 4096,
        *heads,
        pack,
        pack1,
        pack3,
        pack2a,
        pack2b,
    )
    other_projected = other_core(projected)
    activation, mid_stream = call(
        ff_in_kernel,
        (
            jax.ShapeDtypeStruct((rows, ff_in.shape[1]), bf16),
            jax.ShapeDtypeStruct((share, stream.shape[1]), jnp.float32),
        ),
        [pltpu.VMEM((rows, 2048), bf16), pltpu.VMEM((rows, 2048), bf16)],
        2 * rows * 2048 * 1024,
        rows * 10000 + 2048 * 2048,
        where,
        projected,
        other_projected,
        own_stream,
        other_stream,
        norm_gain[None, :],
        *lines,
        scalars=1,
    )
    keep, send = call(
        ff_out_kernel,
        (
            jax.ShapeDtypeStruct((rows // 2, 2048), jnp.float32),
            jax.ShapeDtypeStruct((rows // 2, 2048), bf16),
        ),
        [],
        2 * rows * 2048 * hidden,
        rows * 5000 + 4096 * hidden,
        where,
        activation,
        *lines,
        scalars=1,
    )
    summed = keep + other_core(send).astype(jnp.float32)
    mixed = summed[0:share]
    for i, s in enumerate(SHIFTS):
        block = summed[(i + 1) * share : (i + 2) * share].astype(bf16)
        mixed = mixed + along_x(block, -s).astype(jnp.float32)
    return (mid_stream + mixed).astype(bf16)


def solution(mesh):
    placed = (
        P(("sp", "tp"), None),
        P("sp", "tp", None),
        P("sp", "tp", None),
        P("sp", None),
        P("sp", None),
        P(),
        P(None, "tp", None),
        P(None, "tp", None),
        P("tp"),
        P("tp", None),
        P(),
        P("sp", "tp"),
        P("tp", "sp"),
    )

    return jax.shard_map(
        body, mesh=mesh, in_specs=placed, out_specs=P(("sp", "tp"), None), check_vma=False
    )
```

```python
import functools
import math

import jax
import jax.numpy as jnp
import numpy as np
from jax import lax
from jax.experimental import pallas as pl
from jax.experimental.pallas import tpu as pltpu
from jax.sharding import PartitionSpec as P


HEADS = 16
NOPE = 128
ROPE = 64
LATENT = 512
VDIM = 128
RING = 4
SHARE = 48
SHIFTS = (1, 3, 2)

EPS = 1e-06
THETA = 10000.0
SCALE2 = math.log2(math.e) / math.sqrt(NOPE + ROPE)
LAST_LAST = (((1,), (1,)), ((), ()))


def sp_of(z, y):
    return (z % RING) * RING + (y % RING)


def along(line, values, shift):
    pairs = []
    for z in range(RING):
        for y in range(RING):
            for t in range(2 * RING):
                on_y = (line == "a") == (t % 2 == 0)
                to = sp_of(z, y + shift) if on_y else sp_of(z + shift, y)
                pairs.append((sp_of(z, y) * 2 * RING + t, to * 2 * RING + t))
    return lax.ppermute(values, ("sp", "tp"), pairs)


def along_x(values, shift):
    pairs = [(2 * x + c, 2 * ((x + shift) % RING) + c) for x in range(RING) for c in range(2)]
    return lax.ppermute(values, "tp", pairs)


def other_core(values):
    return lax.ppermute(values, "tp", [(t, t ^ 1) for t in range(2 * RING)])


def dot32(a, b, dims=None):
    if dims is None:
        return jnp.dot(a, b, preferred_element_type=jnp.float32)
    return lax.dot_general(a, b, dims, preferred_element_type=jnp.float32)


def call(kernel, outs, scratch, flops, moved, *args, scalars=0):
    vmem = pl.BlockSpec(memory_space=pltpu.VMEM)
    smem = pl.BlockSpec(memory_space=pltpu.SMEM)
    return pl.pallas_call(
        kernel,
        out_shape=outs,
        in_specs=[smem] * scalars + [vmem] * (len(args) - scalars),
        out_specs=jax.tree.map(lambda _: vmem, outs),
        scratch_shapes=scratch,
        compiler_params=pltpu.CompilerParams(vmem_limit_bytes=24 * 1024 * 1024),
        cost_estimate=pl.CostEstimate(flops=flops, bytes_accessed=moved, transcendentals=0),
    )(*args)


def join_kernel(a_ref, b_ref, c_ref, d_ref, o_ref):
    for i, ref in enumerate((a_ref, b_ref, c_ref, d_ref)):
        o_ref[i] = ref[...]


def join(parts):
    shape = parts[0].shape
    moved = 16 * shape[0] * shape[1]
    return call(join_kernel, jax.ShapeDtypeStruct((4, *shape), parts[0].dtype), [], moved, moved, *parts)


def angles(start, rows):
    values = np.power(np.float32(THETA), -np.arange(0, ROPE, 2, dtype=np.float32) / ROPE)
    index = lax.broadcasted_iota(jnp.int32, (ROPE // 2, 1), 0)
    inverse = jnp.zeros((ROPE // 2, 1), jnp.float32)
    for i, value in enumerate(values):
        inverse = jnp.where(index == i, float(value), inverse)
    token = (start + lax.broadcasted_iota(jnp.int32, (1, rows), 1)).astype(jnp.float32)
    angle = inverse * token
    return jnp.cos(angle), jnp.sin(angle)


def rotated(ref, at, cosine, sine):
    pairs = ROPE // 2
    low = ref[at : at + pairs, :].astype(jnp.float32)
    high = ref[at + pairs : at + ROPE, :].astype(jnp.float32)
    return [low * cosine - high * sine, low * sine + high * cosine]


def keys_kernel(where_ref, latent_ref, key_ref, gain_ref, k_ref, cos_ref, sin_ref):
    rows = k_ref.shape[0]
    cosine, sine = angles(where_ref[4], rows)
    cos_ref[...] = cosine
    sin_ref[...] = sine
    zeros = jnp.zeros((ROPE, rows), jnp.float32)
    keys = jnp.concatenate(rotated(key_ref, 0, cosine, sine) + [zeros], axis=0)
    k_ref[:, LATENT : LATENT + 128] = jnp.transpose(keys).astype(jnp.bfloat16)
    lat = latent_ref[...].astype(jnp.float32)
    mean = jnp.mean(lat * lat, axis=1, keepdims=True)
    k_ref[:, 0:LATENT] = (lat * lax.rsqrt(mean + EPS) * gain_ref[...]).astype(jnp.bfloat16)


def pack_kernel(in_ref, out_ref, pack_ref):
    hidden = out_ref.shape[0]
    pack_ref[0:hidden, :] = out_ref[...]
    for n in range(hidden // 128):
        pack_ref[hidden + n * 128 : hidden + (n + 1) * 128, :] = in_ref[:, n * 128 : (n + 1) * 128]


def queries_kernel(nope_ref, rope_ref, cos_ref, sin_ref, q_ref):
    cosine, sine = cos_ref[...], sin_ref[...]
    parts = rotated(rope_ref, 0, cosine, sine) + rotated(rope_ref, ROPE, cosine, sine)
    q_ref[:, 0:256] = nope_ref[...]
    q_ref[:, 256:384] = jnp.transpose(jnp.concatenate(parts, axis=0)).astype(jnp.bfloat16)


def attend_kernel(q_ref, k_ref, kup_ref, vup_ref, o_ref, qs):
    rows = q_ref.shape[0]
    lane = lax.broadcasted_iota(jnp.int32, (rows, 128), 1)

    def head(h, stats):
        cols = pl.ds(pl.multiple_of(h * 128, 128), 128)
        rot = q_ref[:, 256:384].astype(jnp.float32)
        rot = jnp.where(h == 0, rot, pltpu.roll(rot, ROPE, 1))
        qs[:, 512:640] = jnp.where(lane < ROPE, rot, 0.0).astype(jnp.bfloat16)
        qs[:, 0:512] = dot32(q_ref[:, cols], kup_ref[h], LAST_LAST).astype(jnp.bfloat16)
        scores = dot32(qs[...], k_ref[...], LAST_LAST)
        top = jnp.max(scores, axis=1, keepdims=True) * SCALE2
        expo = jnp.exp2(scores * SCALE2 - top)
        total = jnp.sum(expo, axis=1, keepdims=True)
        out = dot32(expo.astype(jnp.bfloat16), k_ref[:, 0:512])
        out = (out / total).astype(jnp.bfloat16)
        o_ref[:, cols] = dot32(out, vup_ref[h]).astype(jnp.bfloat16)
        lse = top + jnp.log2(total)
        high = lse.astype(jnp.bfloat16).astype(jnp.float32)
        mid = (lse - high).astype(jnp.bfloat16).astype(jnp.float32)
        low = lse - high - mid
        stats = jnp.where(lane == 3 * h, high, stats)
        stats = jnp.where(lane == 3 * h + 1, mid, stats)
        return jnp.where(lane == 3 * h + 2, low, stats)

    stats = lax.fori_loop(0, 2, head, jnp.zeros((rows, 128), jnp.float32))
    o_ref[:, 256:384] = stats.astype(jnp.bfloat16)


def attend(queries, keys, kup, vup):
    rows = queries.shape[0]
    count = keys.shape[0]
    return call(
        attend_kernel,
        jax.ShapeDtypeStruct((rows, 384), jnp.bfloat16),
        [pltpu.VMEM((rows, 640), jnp.bfloat16)],
        2 * 2 * rows * count * 1280,
        count * 1280 + rows * 1536,
        queries,
        keys,
        kup,
        vup,
    )


def combine_kernel(a_ref, b_ref, c_ref, d_ref, h_ref):
    rows = a_ref.shape[0]
    lane = lax.broadcasted_iota(jnp.int32, (rows, 128), 1)
    parts = (a_ref, b_ref, c_ref, d_ref)
    stats = [ref[:, 256:384].astype(jnp.float32) for ref in parts]
    for h in range(2):
        mine = (lane >= 3 * h) & (lane < 3 * h + 3)
        lses = [jnp.sum(jnp.where(mine, s, 0.0), axis=1, keepdims=True) for s in stats]
        top = functools.reduce(jnp.maximum, lses)
        shares = [jnp.exp2(v - top) for v in lses]
        whole = shares[0] + shares[1] + shares[2] + shares[3]
        cols = slice(h * 128, (h + 1) * 128)
        summed = sum(s * ref[:, cols].astype(jnp.float32) for s, ref in zip(shares, parts))
        h_ref[:, cols] = (summed / whole).astype(jnp.bfloat16)


def project_kernel(h0, h1, h2, h3, w0, w1, w2, w3, out_ref):
    heads = (h0, h1, h2, h3)
    rows = h0.shape[0]
    for n in range(4):
        cols = slice(n * 512, (n + 1) * 512)
        total = sum(
            dot32(h[...], w[SHARE : SHARE + 256, cols]) for h, w in zip(heads, (w0, w1, w2, w3))
        )
        out_ref[:, cols] = total.astype(jnp.bfloat16)
    squares = sum(
        jnp.sum(jnp.square(h[...].astype(jnp.float32)), axis=1, keepdims=True) for h in heads
    )
    high = squares.astype(jnp.bfloat16).astype(jnp.float32)
    mid = (squares - high).astype(jnp.bfloat16).astype(jnp.float32)
    low = squares - high - mid
    lane = lax.broadcasted_iota(jnp.int32, (rows, 128), 1)
    stats = jnp.where(lane == 0, high, jnp.where(lane == 1, mid, jnp.where(lane == 2, low, 0.0)))
    out_ref[:, 2048:2176] = stats.astype(jnp.bfloat16)


def ff_in_kernel(
    where_ref, own_ref, oth_ref, sa_ref, sb_ref, gain_ref, w0, w1, w2, w3a, w3b,
    act_ref, mid_ref, xs, xr,
):
    share = mid_ref.shape[0]
    x, c = where_ref[0], where_ref[1]
    gain = gain_ref[...]
    for i in range(8):
        shift = (0, *SHIFTS)[i % 4]
        core = c if i < 4 else 1 - c
        block = lax.rem(x + RING - shift, RING) * 2 + core
        rows = pl.ds(pl.multiple_of(block * share, 16), share)
        both = own_ref[rows, :].astype(jnp.float32) + oth_ref[rows, :].astype(jnp.float32)
        squares = jnp.sum(both[:, 2048:2176], axis=1, keepdims=True)
        scale = lax.rsqrt(squares / (HEADS * VDIM) + EPS)
        at = (i % 4) * share
        stream = (sa_ref if i < 4 else sb_ref)[at : at + share, :]
        mid = stream.astype(jnp.float32) + scale * both[:, 0:2048]
        if i == 0:
            mid_ref[...] = mid
        mean = jnp.mean(mid * mid, axis=1, keepdims=True)
        xs[i * share : (i + 1) * share, :] = (mid * lax.rsqrt(mean + EPS) * gain).astype(jnp.bfloat16)
    for i, block in enumerate(blocks_of(where_ref)):
        cols = pl.ds(pl.multiple_of(block * 128, 128), 128)
        xr[:, i * 128 : (i + 1) * 128] = xs[:, cols]
    hidden = act_ref.shape[1]
    pieces = [(w, k) for w in (w0, w1, w2, w3a, w3b) for k in range(w.shape[0])]
    for n in range(0, hidden // 128, 2):
        columns = []
        for m in (n, n + 1):
            at = hidden + m * 128
            columns.append(jnp.concatenate([w[k, at : at + 128, :] for w, k in pieces], axis=0))
        total = dot32(xr[...], jnp.concatenate(columns, axis=1))
        act_ref[:, n * 128 : (n + 2) * 128] = jnp.square(jnp.maximum(total, 0.0)).astype(jnp.bfloat16)


def blocks_of(where_ref):
    core, z, y = where_ref[1], where_ref[2], where_ref[3]
    order = (0, *SHIFTS)
    blocks = []
    for outer in order:
        for inner in order:
            dz = jnp.where(core == 0, outer, inner)
            dy = jnp.where(core == 0, inner, outer)
            blocks.append(lax.rem(z + RING - dz, RING) * RING + lax.rem(y + RING - dy, RING))
    return blocks


def ff_out_kernel(where_ref, act_ref, w0, w1, w2, w3a, w3b, keep_ref, send_ref):
    half = keep_ref.shape[0]
    hidden = act_ref.shape[1]
    blocks = blocks_of(where_ref)
    pieces = [(w, k) for w in (w0, w1, w2, w3a, w3b) for k in range(w.shape[0])]
    for i in range(0, len(pieces), 2):
        both = jnp.concatenate([w[k, 0:hidden, :] for w, k in pieces[i : i + 2]], axis=1)
        out = dot32(act_ref[...], both)
        for k in range(2):
            cols = pl.ds(pl.multiple_of(blocks[i + k] * 128, 128), 128)
            keep_ref[:, cols] = out[0:half, k * 128 : (k + 1) * 128]
            send_ref[:, cols] = out[half:, k * 128 : (k + 1) * 128].astype(jnp.bfloat16)


def body(
    stream,
    query_nope,
    query_rope,
    latent,
    rope_key,
    latent_gain,
    key_up,
    value_up,
    out_gain,
    out_weight,
    norm_gain,
    ff_in,
    ff_out,
):
    bf16 = jnp.bfloat16
    rows = query_nope.shape[0]
    share = stream.shape[0]
    sp, tp = lax.axis_index("sp"), lax.axis_index("tp")
    where = jnp.stack([tp // 2, tp % 2, sp // RING, sp % RING, sp * rows]).astype(jnp.int32)

    keys, cosine, sine = call(
        keys_kernel,
        (
            jax.ShapeDtypeStruct((rows, 640), bf16),
            jax.ShapeDtypeStruct((ROPE // 2, rows), jnp.float32),
            jax.ShapeDtypeStruct((ROPE // 2, rows), jnp.float32),
        ),
        [],
        rows * 2048,
        rows * 2048,
        where,
        latent,
        jnp.transpose(rope_key),
        latent_gain[None, :],
        scalars=1,
    )
    queries = call(
        queries_kernel,
        jax.ShapeDtypeStruct((rows, 384), bf16),
        [],
        rows * 2048,
        rows * 2048,
        query_nope.reshape(rows, 2 * NOPE),
        jnp.transpose(query_rope, (1, 2, 0)).reshape(2 * ROPE, rows),
        cosine,
        sine,
    )
    kup = jnp.transpose(key_up, (1, 0, 2))
    vup = jnp.transpose(value_up, (1, 0, 2))
    all_keys = jnp.concatenate([keys] + [along("b", keys, s) for s in SHIFTS], axis=0)
    far_queries = [along("a", queries, s) for s in SHIFTS]

    scaled_weight = (out_weight.astype(jnp.float32) * out_gain[:, None]).astype(bf16)
    pack = jnp.concatenate([stream, scaled_weight], axis=0)
    packs = [pack] + [along_x(pack, s) for s in SHIFTS]
    own_stream = jnp.concatenate([p[:share] for p in packs], axis=0)
    other_stream = other_core(own_stream)

    hidden = ff_in.shape[1]
    weights = call(
        pack_kernel,
        jax.ShapeDtypeStruct((2 * hidden, 128), bf16),
        [],
        hidden * 128,
        hidden * 1024,
        ff_in,
        ff_out,
    )
    line = join([weights] + [along("a", weights, s) for s in SHIFTS])
    line1, line3 = along("b", line, 1), along("b", line, 3)
    line2a, line2b = along("b", line1[:2], 1), along("b", line3[2:], 3)
    lines = (line, line1, line3, line2a, line2b)

    backs = []
    for s, q in zip(SHIFTS, far_queries):
        backs.append(along("a", attend(q, all_keys, kup, vup), -s))
    mine = attend(queries, all_keys, kup, vup)
    head_out = call(
        combine_kernel,
        jax.ShapeDtypeStruct((rows, 256), bf16),
        [],
        rows * 256 * 16,
        rows * 384 * 2 * 5,
        mine,
        *backs,
    )
    heads = [head_out] + [along_x(head_out, s) for s in SHIFTS]
    projected = call(
        project_kernel,
        jax.ShapeDtypeStruct((rows, 2176), bf16),
        [],
        2 * rows * 1024 * 2048,
        rows * 6400 + 1024 * 4096,
        *heads,
        *packs,
    )
    other_projected = other_core(projected)
    activation, mid_stream = call(
        ff_in_kernel,
        (
            jax.ShapeDtypeStruct((rows, ff_in.shape[1]), bf16),
            jax.ShapeDtypeStruct((share, stream.shape[1]), jnp.float32),
        ),
        [pltpu.VMEM((rows, 2048), bf16), pltpu.VMEM((rows, 2048), bf16)],
        2 * rows * 2048 * 1024,
        rows * 10000 + 2048 * 2048,
        where,
        projected,
        other_projected,
        own_stream,
        other_stream,
        norm_gain[None, :],
        *lines,
        scalars=1,
    )
    keep, send = call(
        ff_out_kernel,
        (
            jax.ShapeDtypeStruct((rows // 2, 2048), jnp.float32),
            jax.ShapeDtypeStruct((rows // 2, 2048), bf16),
        ),
        [],
        2 * rows * 2048 * hidden,
        rows * 5000 + 4096 * hidden,
        where,
        activation,
        *lines,
        scalars=1,
    )
    summed = keep + other_core(send).astype(jnp.float32)
    mixed = summed[0:share]
    for i, s in enumerate(SHIFTS):
        block = summed[(i + 1) * share : (i + 2) * share].astype(bf16)
        mixed = mixed + along_x(block, -s).astype(jnp.float32)
    return (mid_stream + mixed).astype(bf16)


def solution(mesh):
    placed = (
        P(("sp", "tp"), None),
        P("sp", "tp", None),
        P("sp", "tp", None),
        P("sp", None),
        P("sp", None),
        P(),
        P(None, "tp", None),
        P(None, "tp", None),
        P("tp"),
        P("tp", None),
        P(),
        P("sp", "tp"),
        P("tp", "sp"),
    )

    return jax.shard_map(
        body, mesh=mesh, in_specs=placed, out_specs=P(("sp", "tp"), None), check_vma=False
    )
```

```python
import functools
import math

import jax
import jax.numpy as jnp
import numpy as np
from jax import lax
from jax.experimental import pallas as pl
from jax.experimental.pallas import tpu as pltpu
from jax.sharding import PartitionSpec as P


HEADS = 16
NOPE = 128
ROPE = 64
LATENT = 512
VDIM = 128
RING = 4
SHARE = 48
SHIFTS = (1, 3, 2)

EPS = 1e-06
THETA = 10000.0
SCALE2 = math.log2(math.e) / math.sqrt(NOPE + ROPE)
LAST_LAST = (((1,), (1,)), ((), ()))


def sp_of(z, y):
    return (z % RING) * RING + (y % RING)


def along(line, values, shift):
    pairs = []
    for z in range(RING):
        for y in range(RING):
            for t in range(2 * RING):
                on_y = (line == "a") == (t % 2 == 0)
                to = sp_of(z, y + shift) if on_y else sp_of(z + shift, y)
                pairs.append((sp_of(z, y) * 2 * RING + t, to * 2 * RING + t))
    return lax.ppermute(values, ("sp", "tp"), pairs)


def along_y(values, shift):
    pairs = [(sp_of(z, y), sp_of(z, y + shift)) for z in range(RING) for y in range(RING)]
    return lax.ppermute(values, "sp", pairs)


def up_and_down(values):
    pairs = []
    for z in range(RING):
        for y in range(RING):
            for t in range(2 * RING):
                to = sp_of(z + (1 if t % 2 == 0 else -1), y)
                pairs.append((sp_of(z, y) * 2 * RING + t, to * 2 * RING + t))
    return lax.ppermute(values, ("sp", "tp"), pairs)


def two_up(values):
    pairs = [(sp_of(z, y), sp_of(z + 2, y)) for z in range(RING) for y in range(RING)]
    return lax.ppermute(values, "sp", pairs)


def along_x(values, shift):
    pairs = [(2 * x + c, 2 * ((x + shift) % RING) + c) for x in range(RING) for c in range(2)]
    return lax.ppermute(values, "tp", pairs)


def other_core(values):
    return lax.ppermute(values, "tp", [(t, t ^ 1) for t in range(2 * RING)])


def dot32(a, b, dims=None):
    if dims is None:
        return jnp.dot(a, b, preferred_element_type=jnp.float32)
    return lax.dot_general(a, b, dims, preferred_element_type=jnp.float32)


def call(kernel, outs, scratch, flops, moved, *args, scalars=0):
    vmem = pl.BlockSpec(memory_space=pltpu.VMEM)
    smem = pl.BlockSpec(memory_space=pltpu.SMEM)
    return pl.pallas_call(
        kernel,
        out_shape=outs,
        in_specs=[smem] * scalars + [vmem] * (len(args) - scalars),
        out_specs=jax.tree.map(lambda _: vmem, outs),
        scratch_shapes=scratch,
        compiler_params=pltpu.CompilerParams(vmem_limit_bytes=24 * 1024 * 1024),
        cost_estimate=pl.CostEstimate(flops=flops, bytes_accessed=moved, transcendentals=0),
    )(*args)


def join_kernel(a_ref, b_ref, c_ref, d_ref, in_ref, out_ref):
    hidden = in_ref.shape[1]
    for i, ref in enumerate((a_ref, b_ref, c_ref, d_ref)):
        out_ref[i] = ref[0:hidden, :]
        in_ref[i] = ref[hidden:, :]


def join(packs):
    hidden = packs[0].shape[0] // 2
    half = jax.ShapeDtypeStruct((4, hidden, 128), packs[0].dtype)
    moved = 32 * hidden * 128
    return call(join_kernel, (half, half), [], moved, moved, *packs)


def angles(start, rows):
    values = np.power(np.float32(THETA), -np.arange(0, ROPE, 2, dtype=np.float32) / ROPE)
    index = lax.broadcasted_iota(jnp.int32, (ROPE // 2, 1), 0)
    inverse = jnp.zeros((ROPE // 2, 1), jnp.float32)
    for i, value in enumerate(values):
        inverse = jnp.where(index == i, float(value), inverse)
    token = (start + lax.broadcasted_iota(jnp.int32, (1, rows), 1)).astype(jnp.float32)
    angle = inverse * token
    return jnp.cos(angle), jnp.sin(angle)


def rotated(ref, at, cosine, sine):
    pairs = ROPE // 2
    low = ref[at : at + pairs, :].astype(jnp.float32)
    high = ref[at + pairs : at + ROPE, :].astype(jnp.float32)
    return [low * cosine - high * sine, low * sine + high * cosine]


def keys_kernel(where_ref, latent_ref, key_ref, gain_ref, k_ref, half_ref, cos_ref, sin_ref):
    rows = k_ref.shape[0]
    cosine, sine = angles(where_ref[4], rows)
    cos_ref[...] = cosine
    sin_ref[...] = sine
    zeros = jnp.zeros((ROPE, rows), jnp.float32)
    keys = jnp.concatenate(rotated(key_ref, 0, cosine, sine) + [zeros], axis=0)
    k_ref[:, LATENT : LATENT + 128] = jnp.transpose(keys).astype(jnp.bfloat16)
    lat = latent_ref[...].astype(jnp.float32)
    mean = jnp.mean(lat * lat, axis=1, keepdims=True)
    k_ref[:, 0:LATENT] = (lat * lax.rsqrt(mean + EPS) * gain_ref[...]).astype(jnp.bfloat16)
    half = rows // 2
    half_ref[...] = k_ref[pl.ds(pl.multiple_of(where_ref[1] * half, 64), half), :]


def pack_kernel(in_ref, out_ref, pack_ref):
    hidden = out_ref.shape[0]
    pack_ref[0:hidden, :] = out_ref[...]
    for n in range(hidden // 128):
        pack_ref[hidden + n * 128 : hidden + (n + 1) * 128, :] = in_ref[:, n * 128 : (n + 1) * 128]


def queries_kernel(nope_ref, rope_ref, cos_ref, sin_ref, q_ref):
    cosine, sine = cos_ref[...], sin_ref[...]
    parts = rotated(rope_ref, 0, cosine, sine) + rotated(rope_ref, ROPE, cosine, sine)
    q_ref[:, 0:256] = nope_ref[...]
    q_ref[:, 256:384] = jnp.transpose(jnp.concatenate(parts, axis=0)).astype(jnp.bfloat16)


def attend_kernel(q_ref, k_ref, kup_ref, vup_ref, o_ref, qs):
    rows = q_ref.shape[0]
    lane = lax.broadcasted_iota(jnp.int32, (rows, 128), 1)

    def head(h, stats):
        cols = slice(h * 128, (h + 1) * 128)
        rot = q_ref[:, 256:384].astype(jnp.float32)
        rot = pltpu.roll(rot, ROPE, 1) if h else rot
        qs[h, :, 512:640] = jnp.where(lane < ROPE, rot, 0.0).astype(jnp.bfloat16)
        qs[h, :, 0:512] = dot32(q_ref[:, cols], kup_ref[h], LAST_LAST).astype(jnp.bfloat16)
        scores = dot32(qs[h], k_ref[...], LAST_LAST)
        top = jnp.max(scores, axis=1, keepdims=True) * SCALE2
        expo = jnp.exp2(scores * SCALE2 - top)
        total = jnp.sum(expo, axis=1, keepdims=True)
        out = dot32(expo.astype(jnp.bfloat16), k_ref[:, 0:512])
        out = (out / total).astype(jnp.bfloat16)
        o_ref[:, cols] = dot32(out, vup_ref[h]).astype(jnp.bfloat16)
        lse = top + jnp.log2(total)
        high = lse.astype(jnp.bfloat16).astype(jnp.float32)
        mid = (lse - high).astype(jnp.bfloat16).astype(jnp.float32)
        low = lse - high - mid
        stats = jnp.where(lane == 3 * h, high, stats)
        stats = jnp.where(lane == 3 * h + 1, mid, stats)
        return jnp.where(lane == 3 * h + 2, low, stats)

    stats = head(1, head(0, jnp.zeros((rows, 128), jnp.float32)))
    o_ref[:, 256:384] = stats.astype(jnp.bfloat16)


def attend(queries, keys, kup, vup):
    rows = queries.shape[0]
    count = keys.shape[0]
    return call(
        attend_kernel,
        jax.ShapeDtypeStruct((rows, 384), jnp.bfloat16),
        [pltpu.VMEM((2, rows, 640), jnp.bfloat16)],
        2 * 2 * rows * count * 1280,
        count * 1280 + rows * 1536,
        queries,
        keys,
        kup,
        vup,
    )


def combine_kernel(a_ref, b_ref, c_ref, d_ref, h_ref):
    rows = a_ref.shape[0]
    lane = lax.broadcasted_iota(jnp.int32, (rows, 128), 1)
    parts = (a_ref, b_ref, c_ref, d_ref)
    stats = [ref[:, 256:384].astype(jnp.float32) for ref in parts]
    for h in range(2):
        mine = (lane >= 3 * h) & (lane < 3 * h + 3)
        lses = [jnp.sum(jnp.where(mine, s, 0.0), axis=1, keepdims=True) for s in stats]
        top = functools.reduce(jnp.maximum, lses)
        shares = [jnp.exp2(v - top) for v in lses]
        whole = shares[0] + shares[1] + shares[2] + shares[3]
        cols = slice(h * 128, (h + 1) * 128)
        summed = sum(s * ref[:, cols].astype(jnp.float32) for s, ref in zip(shares, parts))
        h_ref[:, cols] = (summed / whole).astype(jnp.bfloat16)


def project_kernel(h0, h1, h2, h3, w0, w1, w2, w3, out_ref):
    heads = (h0, h1, h2, h3)
    rows = h0.shape[0]
    for n in range(4):
        cols = slice(n * 512, (n + 1) * 512)
        total = sum(
            dot32(h[...], w[SHARE : SHARE + 256, cols]) for h, w in zip(heads, (w0, w1, w2, w3))
        )
        out_ref[:, cols] = total.astype(jnp.bfloat16)
    squares = sum(
        jnp.sum(jnp.square(h[...].astype(jnp.float32)), axis=1, keepdims=True) for h in heads
    )
    high = squares.astype(jnp.bfloat16).astype(jnp.float32)
    mid = (squares - high).astype(jnp.bfloat16).astype(jnp.float32)
    low = squares - high - mid
    lane = lax.broadcasted_iota(jnp.int32, (rows, 128), 1)
    stats = jnp.where(lane == 0, high, jnp.where(lane == 1, mid, jnp.where(lane == 2, low, 0.0)))
    out_ref[:, 2048:2176] = stats.astype(jnp.bfloat16)


def ff_in_kernel(
    where_ref, own_ref, oth_ref, sa_ref, sb_ref, gain_ref, w0, w1, w2, w3a, w3b,
    act_ref, mid_ref, xs, xr,
):
    share = mid_ref.shape[0]
    x, c = where_ref[0], where_ref[1]
    gain = gain_ref[...]
    for i in range(8):
        shift = (0, *SHIFTS)[i % 4]
        core = c if i < 4 else 1 - c
        block = lax.rem(x + RING - shift, RING) * 2 + core
        rows = pl.ds(pl.multiple_of(block * share, 16), share)
        both = own_ref[rows, :].astype(jnp.float32) + oth_ref[rows, :].astype(jnp.float32)
        squares = jnp.sum(both[:, 2048:2176], axis=1, keepdims=True)
        scale = lax.rsqrt(squares / (HEADS * VDIM) + EPS)
        at = (i % 4) * share
        stream = (sa_ref if i < 4 else sb_ref)[at : at + share, :]
        mid = stream.astype(jnp.float32) + scale * both[:, 0:2048]
        if i == 0:
            mid_ref[...] = mid
        mean = jnp.mean(mid * mid, axis=1, keepdims=True)
        xs[i * share : (i + 1) * share, :] = (mid * lax.rsqrt(mean + EPS) * gain).astype(jnp.bfloat16)
    for i, block in enumerate(blocks_of(where_ref)):
        cols = pl.ds(pl.multiple_of(block * 128, 128), 128)
        xr[:, i * 128 : (i + 1) * 128] = xs[:, cols]
    hidden = act_ref.shape[1]
    pieces = [(w, k) for w in (w0, w1, w2, w3a, w3b) for k in range(w.shape[0])]
    for n in range(0, hidden // 128, 2):
        columns = []
        for m in (n, n + 1):
            at = m * 128
            columns.append(jnp.concatenate([w[k, at : at + 128, :] for w, k in pieces], axis=0))
        total = dot32(xr[...], jnp.concatenate(columns, axis=1))
        act_ref[:, n * 128 : (n + 2) * 128] = jnp.square(jnp.maximum(total, 0.0)).astype(jnp.bfloat16)


def blocks_of(where_ref):
    core, z, y = where_ref[1], where_ref[2], where_ref[3]
    order = (0, *SHIFTS)
    blocks = []
    for outer in order:
        for inner in order:
            dz = jnp.where(core == 0, outer, inner)
            dy = jnp.where(core == 0, inner, outer)
            blocks.append(lax.rem(z + RING - dz, RING) * RING + lax.rem(y + RING - dy, RING))
    return blocks


def ff_out_kernel(where_ref, act_ref, w0, w1, w2, w3a, w3b, keep_ref, send_ref):
    half = keep_ref.shape[0]
    hidden = act_ref.shape[1]
    blocks = blocks_of(where_ref)
    pieces = [(w, k) for w in (w0, w1, w2, w3a, w3b) for k in range(w.shape[0])]
    for i in range(0, len(pieces), 2):
        both = jnp.concatenate([w[k, 0:hidden, :] for w, k in pieces[i : i + 2]], axis=1)
        out = dot32(act_ref[...], both)
        for k in range(2):
            cols = pl.ds(pl.multiple_of(blocks[i + k] * 128, 128), 128)
            keep_ref[:, cols] = out[0:half, k * 128 : (k + 1) * 128]
            send_ref[:, cols] = out[half:, k * 128 : (k + 1) * 128].astype(jnp.bfloat16)


def body(
    stream,
    query_nope,
    query_rope,
    latent,
    rope_key,
    latent_gain,
    key_up,
    value_up,
    out_gain,
    out_weight,
    norm_gain,
    ff_in,
    ff_out,
):
    bf16 = jnp.bfloat16
    rows = query_nope.shape[0]
    share = stream.shape[0]
    sp, tp = lax.axis_index("sp"), lax.axis_index("tp")
    where = jnp.stack([tp // 2, tp % 2, sp // RING, sp % RING, sp * rows]).astype(jnp.int32)

    keys, half_keys, cosine, sine = call(
        keys_kernel,
        (
            jax.ShapeDtypeStruct((rows, 640), bf16),
            jax.ShapeDtypeStruct((rows // 2, 640), bf16),
            jax.ShapeDtypeStruct((ROPE // 2, rows), jnp.float32),
            jax.ShapeDtypeStruct((ROPE // 2, rows), jnp.float32),
        ),
        [],
        rows * 2048,
        rows * 2048,
        where,
        latent,
        jnp.transpose(rope_key),
        latent_gain[None, :],
        scalars=1,
    )
    queries = call(
        queries_kernel,
        jax.ShapeDtypeStruct((rows, 384), bf16),
        [],
        rows * 2048,
        rows * 2048,
        query_nope.reshape(rows, 2 * NOPE),
        jnp.transpose(query_rope, (1, 2, 0)).reshape(2 * ROPE, rows),
        cosine,
        sine,
    )
    kup = jnp.transpose(key_up, (1, 0, 2))
    vup = jnp.transpose(value_up, (1, 0, 2))
    far_keys = jnp.concatenate([up_and_down(keys), two_up(half_keys)], axis=0)
    all_keys = jnp.concatenate([keys, far_keys, other_core(far_keys)], axis=0)
    far_queries = [along_y(queries, s) for s in SHIFTS]

    scaled_weight = (out_weight.astype(jnp.float32) * out_gain[:, None]).astype(bf16)
    pack = jnp.concatenate([stream, scaled_weight], axis=0)
    packs = [pack] + [along_x(pack, s) for s in SHIFTS]
    own_stream = jnp.concatenate([p[:share] for p in packs], axis=0)
    other_stream = other_core(own_stream)

    hidden = ff_in.shape[1]
    weights = call(
        pack_kernel,
        jax.ShapeDtypeStruct((2 * hidden, 128), bf16),
        [],
        hidden * 128,
        hidden * 1024,
        ff_in,
        ff_out,
    )
    line_in, line_out = join([weights] + [along("a", weights, s) for s in SHIFTS])

    def spread(line):
        up, down = along("b", line, 1), along("b", line, 3)
        far_up = along("b", up[:2], 1)
        return line, up, down, far_up, along("b", down[2:], 3)

    in_lines, out_lines = spread(line_in), spread(line_out)

    backs = []
    for s, q in zip(SHIFTS, far_queries):
        backs.append(along_y(attend(q, all_keys, kup, vup), -s))
    mine = attend(queries, all_keys, kup, vup)
    head_out = call(
        combine_kernel,
        jax.ShapeDtypeStruct((rows, 256), bf16),
        [],
        rows * 256 * 16,
        rows * 384 * 2 * 5,
        mine,
        *backs,
    )
    heads = [head_out] + [along_x(head_out, s) for s in SHIFTS]
    projected = call(
        project_kernel,
        jax.ShapeDtypeStruct((rows, 2176), bf16),
        [],
        2 * rows * 1024 * 2048,
        rows * 6400 + 1024 * 4096,
        *heads,
        *packs,
    )
    other_projected = other_core(projected)
    activation, mid_stream = call(
        ff_in_kernel,
        (
            jax.ShapeDtypeStruct((rows, ff_in.shape[1]), bf16),
            jax.ShapeDtypeStruct((share, stream.shape[1]), jnp.float32),
        ),
        [pltpu.VMEM((rows, 2048), bf16), pltpu.VMEM((rows, 2048), bf16)],
        2 * rows * 2048 * 1024,
        rows * 10000 + 2048 * 2048,
        where,
        projected,
        other_projected,
        own_stream,
        other_stream,
        norm_gain[None, :],
        *in_lines,
        scalars=1,
    )
    keep, send = call(
        ff_out_kernel,
        (
            jax.ShapeDtypeStruct((rows // 2, 2048), jnp.float32),
            jax.ShapeDtypeStruct((rows // 2, 2048), bf16),
        ),
        [],
        2 * rows * 2048 * hidden,
        rows * 5000 + 4096 * hidden,
        where,
        activation,
        *out_lines,
        scalars=1,
    )
    summed = keep + other_core(send).astype(jnp.float32)
    mixed = summed[0:share]
    for i, s in enumerate(SHIFTS):
        block = summed[(i + 1) * share : (i + 2) * share].astype(bf16)
        mixed = mixed + along_x(block, -s).astype(jnp.float32)
    return (mid_stream + mixed).astype(bf16)


def solution(mesh):
    placed = (
        P(("sp", "tp"), None),
        P("sp", "tp", None),
        P("sp", "tp", None),
        P("sp", None),
        P("sp", None),
        P(),
        P(None, "tp", None),
        P(None, "tp", None),
        P("tp"),
        P("tp", None),
        P(),
        P("sp", "tp"),
        P("tp", "sp"),
    )

    return jax.shard_map(
        body, mesh=mesh, in_specs=placed, out_specs=P(("sp", "tp"), None), check_vma=False
    )
```

```python
import functools
import math

import jax
import jax.numpy as jnp
import numpy as np
from jax import lax
from jax.experimental import pallas as pl
from jax.experimental.pallas import tpu as pltpu
from jax.sharding import PartitionSpec as P


HEADS = 16
NOPE = 128
ROPE = 64
LATENT = 512
VDIM = 128
RING = 4
SHARE = 48
SHIFTS = (1, 3, 2)

EPS = 1e-06
THETA = 10000.0
SCALE2 = math.log2(math.e) / math.sqrt(NOPE + ROPE)
LAST_LAST = (((1,), (1,)), ((), ()))


def sp_of(z, y):
    return (z % RING) * RING + (y % RING)


def along(line, values, shift):
    pairs = []
    for z in range(RING):
        for y in range(RING):
            for t in range(2 * RING):
                on_y = (line == "a") == (t % 2 == 0)
                to = sp_of(z, y + shift) if on_y else sp_of(z + shift, y)
                pairs.append((sp_of(z, y) * 2 * RING + t, to * 2 * RING + t))
    return lax.ppermute(values, ("sp", "tp"), pairs)


def along_y(values, shift):
    pairs = [(sp_of(z, y), sp_of(z, y + shift)) for z in range(RING) for y in range(RING)]
    return lax.ppermute(values, "sp", pairs)


def up_and_down(values):
    pairs = []
    for z in range(RING):
        for y in range(RING):
            for t in range(2 * RING):
                to = sp_of(z + (1 if t % 2 == 0 else -1), y)
                pairs.append((sp_of(z, y) * 2 * RING + t, to * 2 * RING + t))
    return lax.ppermute(values, ("sp", "tp"), pairs)


def two_up(values):
    pairs = [(sp_of(z, y), sp_of(z + 2, y)) for z in range(RING) for y in range(RING)]
    return lax.ppermute(values, "sp", pairs)


def along_x(values, shift):
    pairs = [(2 * x + c, 2 * ((x + shift) % RING) + c) for x in range(RING) for c in range(2)]
    return lax.ppermute(values, "tp", pairs)


def other_core(values):
    return lax.ppermute(values, "tp", [(t, t ^ 1) for t in range(2 * RING)])


def dot32(a, b, dims=None):
    if dims is None:
        return jnp.dot(a, b, preferred_element_type=jnp.float32)
    return lax.dot_general(a, b, dims, preferred_element_type=jnp.float32)


def call(kernel, outs, scratch, flops, moved, *args, scalars=0):
    vmem = pl.BlockSpec(memory_space=pltpu.VMEM)
    smem = pl.BlockSpec(memory_space=pltpu.SMEM)
    return pl.pallas_call(
        kernel,
        out_shape=outs,
        in_specs=[smem] * scalars + [vmem] * (len(args) - scalars),
        out_specs=jax.tree.map(lambda _: vmem, outs),
        scratch_shapes=scratch,
        compiler_params=pltpu.CompilerParams(vmem_limit_bytes=24 * 1024 * 1024),
        cost_estimate=pl.CostEstimate(flops=flops, bytes_accessed=moved, transcendentals=0),
    )(*args)


def join_kernel(a_ref, b_ref, c_ref, d_ref, in_ref, out_ref):
    hidden = in_ref.shape[1]
    for i, ref in enumerate((a_ref, b_ref, c_ref, d_ref)):
        out_ref[i] = ref[0:hidden, :]
        in_ref[i] = ref[hidden:, :]


def join(packs):
    hidden = packs[0].shape[0] // 2
    half = jax.ShapeDtypeStruct((4, hidden, 128), packs[0].dtype)
    moved = 32 * hidden * 128
    return call(join_kernel, (half, half), [], moved, moved, *packs)


def angles(start, rows):
    values = np.power(np.float32(THETA), -np.arange(0, ROPE, 2, dtype=np.float32) / ROPE)
    index = lax.broadcasted_iota(jnp.int32, (ROPE // 2, 1), 0)
    inverse = jnp.zeros((ROPE // 2, 1), jnp.float32)
    for i, value in enumerate(values):
        inverse = jnp.where(index == i, float(value), inverse)
    token = (start + lax.broadcasted_iota(jnp.int32, (1, rows), 1)).astype(jnp.float32)
    angle = inverse * token
    return jnp.cos(angle), jnp.sin(angle)


def rotated(ref, at, cosine, sine):
    pairs = ROPE // 2
    low = ref[at : at + pairs, :].astype(jnp.float32)
    high = ref[at + pairs : at + ROPE, :].astype(jnp.float32)
    return [low * cosine - high * sine, low * sine + high * cosine]


def keys_kernel(where_ref, latent_ref, key_ref, gain_ref, k_ref, half_ref, cos_ref, sin_ref):
    rows = k_ref.shape[0]
    cosine, sine = angles(where_ref[4], rows)
    cos_ref[...] = cosine
    sin_ref[...] = sine
    zeros = jnp.zeros((ROPE, rows), jnp.float32)
    keys = jnp.concatenate(rotated(key_ref, 0, cosine, sine) + [zeros], axis=0)
    k_ref[:, LATENT : LATENT + 128] = jnp.transpose(keys).astype(jnp.bfloat16)
    lat = latent_ref[...].astype(jnp.float32)
    mean = jnp.mean(lat * lat, axis=1, keepdims=True)
    k_ref[:, 0:LATENT] = (lat * lax.rsqrt(mean + EPS) * gain_ref[...]).astype(jnp.bfloat16)
    half = rows // 2
    half_ref[...] = k_ref[pl.ds(pl.multiple_of(where_ref[1] * half, 64), half), :]


def pack_kernel(in_ref, out_ref, pack_ref):
    hidden = out_ref.shape[0]
    pack_ref[0:hidden, :] = out_ref[...]
    for n in range(hidden // 128):
        pack_ref[hidden + n * 128 : hidden + (n + 1) * 128, :] = in_ref[:, n * 128 : (n + 1) * 128]


def queries_kernel(nope_ref, rope_ref, cos_ref, sin_ref, q_ref):
    cosine, sine = cos_ref[...], sin_ref[...]
    parts = rotated(rope_ref, 0, cosine, sine) + rotated(rope_ref, ROPE, cosine, sine)
    q_ref[:, 0:256] = nope_ref[...]
    q_ref[:, 256:384] = jnp.transpose(jnp.concatenate(parts, axis=0)).astype(jnp.bfloat16)


def attend_kernel(q_ref, kup_ref, vup_ref, *refs):
    key_refs, o_ref, qs = refs[:-2], refs[-2], refs[-1]
    rows = q_ref.shape[0]
    lane = lax.broadcasted_iota(jnp.int32, (rows, 128), 1)

    raw = []
    for h in range(2):
        rot = q_ref[:, 256:384].astype(jnp.float32)
        rot = pltpu.roll(rot, ROPE, 1) if h else rot
        qs[h, :, 512:640] = jnp.where(lane < ROPE, rot, 0.0).astype(jnp.bfloat16)
        cols = slice(h * 128, (h + 1) * 128)
        qs[h, :, 0:512] = dot32(q_ref[:, cols], kup_ref[h], LAST_LAST).astype(jnp.bfloat16)
    for h in range(2):
        raw.append([dot32(qs[h], k[...], LAST_LAST) for k in key_refs])
    stats = jnp.zeros((rows, 128), jnp.float32)
    for h, scores in enumerate(raw):
        tops = [jnp.max(part, axis=1, keepdims=True) for part in scores]
        top = functools.reduce(jnp.maximum, tops) * SCALE2
        total, out = 0.0, 0.0
        for part, k in zip(scores, key_refs):
            expo = jnp.exp2(part * SCALE2 - top)
            total += jnp.sum(expo, axis=1, keepdims=True)
            out += dot32(expo.astype(jnp.bfloat16), k[:, 0:512])
        out = (out / total).astype(jnp.bfloat16)
        o_ref[:, h * 128 : (h + 1) * 128] = dot32(out, vup_ref[h]).astype(jnp.bfloat16)
        lse = top + jnp.log2(total)
        high = lse.astype(jnp.bfloat16).astype(jnp.float32)
        mid = (lse - high).astype(jnp.bfloat16).astype(jnp.float32)
        low = lse - high - mid
        stats = jnp.where(lane == 3 * h, high, stats)
        stats = jnp.where(lane == 3 * h + 1, mid, stats)
        stats = jnp.where(lane == 3 * h + 2, low, stats)
    o_ref[:, 256:384] = stats.astype(jnp.bfloat16)


def attend(queries, keys, kup, vup):
    rows = queries.shape[0]
    count = sum(k.shape[0] for k in keys)
    return call(
        attend_kernel,
        jax.ShapeDtypeStruct((rows, 384), jnp.bfloat16),
        [pltpu.VMEM((2, rows, 640), jnp.bfloat16)],
        2 * 2 * rows * count * 1280,
        count * 1280 + rows * 1536,
        queries,
        kup,
        vup,
        *keys,
    )


def combine_kernel(*refs):
    parts, h_ref = refs[:-1], refs[-1]
    rows = h_ref.shape[0]
    lane = lax.broadcasted_iota(jnp.int32, (rows, 128), 1)
    stats = [ref[:, 256:384].astype(jnp.float32) for ref in parts]
    for h in range(2):
        mine = (lane >= 3 * h) & (lane < 3 * h + 3)
        lses = [jnp.sum(jnp.where(mine, s, 0.0), axis=1, keepdims=True) for s in stats]
        top = functools.reduce(jnp.maximum, lses)
        shares = [jnp.exp2(v - top) for v in lses]
        whole = sum(shares)
        cols = slice(h * 128, (h + 1) * 128)
        summed = sum(s * ref[:, cols].astype(jnp.float32) for s, ref in zip(shares, parts))
        h_ref[:, cols] = (summed / whole).astype(jnp.bfloat16)


def project_kernel(h0, h1, h2, h3, w0, w1, w2, w3, out_ref):
    heads = (h0, h1, h2, h3)
    rows = h0.shape[0]
    for n in range(4):
        cols = slice(n * 512, (n + 1) * 512)
        total = sum(
            dot32(h[...], w[SHARE : SHARE + 256, cols]) for h, w in zip(heads, (w0, w1, w2, w3))
        )
        out_ref[:, cols] = total.astype(jnp.bfloat16)
    squares = sum(
        jnp.sum(jnp.square(h[...].astype(jnp.float32)), axis=1, keepdims=True) for h in heads
    )
    high = squares.astype(jnp.bfloat16).astype(jnp.float32)
    mid = (squares - high).astype(jnp.bfloat16).astype(jnp.float32)
    low = squares - high - mid
    lane = lax.broadcasted_iota(jnp.int32, (rows, 128), 1)
    stats = jnp.where(lane == 0, high, jnp.where(lane == 1, mid, jnp.where(lane == 2, low, 0.0)))
    out_ref[:, 2048:2176] = stats.astype(jnp.bfloat16)


def ff_in_kernel(
    where_ref, own_ref, oth_ref, sa_ref, sb_ref, gain_ref, w0, w1, w2, w3a, w3b,
    act_ref, mid_ref, xs, xr,
):
    share = mid_ref.shape[0]
    x, c = where_ref[0], where_ref[1]
    gain = gain_ref[...]
    for i in range(8):
        shift = (0, *SHIFTS)[i % 4]
        core = c if i < 4 else 1 - c
        block = lax.rem(x + RING - shift, RING) * 2 + core
        rows = pl.ds(pl.multiple_of(block * share, 16), share)
        both = own_ref[rows, :].astype(jnp.float32) + oth_ref[rows, :].astype(jnp.float32)
        squares = jnp.sum(both[:, 2048:2176], axis=1, keepdims=True)
        scale = lax.rsqrt(squares / (HEADS * VDIM) + EPS)
        at = (i % 4) * share
        stream = (sa_ref if i < 4 else sb_ref)[at : at + share, :]
        mid = stream.astype(jnp.float32) + scale * both[:, 0:2048]
        if i == 0:
            mid_ref[...] = mid
        mean = jnp.mean(mid * mid, axis=1, keepdims=True)
        xs[i * share : (i + 1) * share, :] = (mid * lax.rsqrt(mean + EPS) * gain).astype(jnp.bfloat16)
    for i, block in enumerate(blocks_of(where_ref)):
        cols = pl.ds(pl.multiple_of(block * 128, 128), 128)
        xr[:, i * 128 : (i + 1) * 128] = xs[:, cols]
    hidden = act_ref.shape[1]
    pieces = [(w, k) for w in (w0, w1, w2, w3a, w3b) for k in range(w.shape[0])]
    for n in range(0, hidden // 128, 2):
        columns = []
        for m in (n, n + 1):
            at = m * 128
            columns.append(jnp.concatenate([w[k, at : at + 128, :] for w, k in pieces], axis=0))
        total = dot32(xr[...], jnp.concatenate(columns, axis=1))
        act_ref[:, n * 128 : (n + 2) * 128] = jnp.square(jnp.maximum(total, 0.0)).astype(jnp.bfloat16)


def blocks_of(where_ref):
    core, z, y = where_ref[1], where_ref[2], where_ref[3]
    order = (0, *SHIFTS)
    blocks = []
    for outer in order:
        for inner in order:
            dz = jnp.where(core == 0, outer, inner)
            dy = jnp.where(core == 0, inner, outer)
            blocks.append(lax.rem(z + RING - dz, RING) * RING + lax.rem(y + RING - dy, RING))
    return blocks


def ff_out_kernel(where_ref, act_ref, w0, w1, w2, w3a, w3b, keep_ref, send_ref):
    half = keep_ref.shape[0]
    hidden = act_ref.shape[1]
    blocks = blocks_of(where_ref)
    pieces = [(w, k) for w in (w0, w1, w2, w3a, w3b) for k in range(w.shape[0])]
    for i in range(0, len(pieces), 2):
        both = jnp.concatenate([w[k, 0:hidden, :] for w, k in pieces[i : i + 2]], axis=1)
        out = dot32(act_ref[...], both)
        for k in range(2):
            cols = pl.ds(pl.multiple_of(blocks[i + k] * 128, 128), 128)
            keep_ref[:, cols] = out[0:half, k * 128 : (k + 1) * 128]
            send_ref[:, cols] = out[half:, k * 128 : (k + 1) * 128].astype(jnp.bfloat16)


def body(
    stream,
    query_nope,
    query_rope,
    latent,
    rope_key,
    latent_gain,
    key_up,
    value_up,
    out_gain,
    out_weight,
    norm_gain,
    ff_in,
    ff_out,
):
    bf16 = jnp.bfloat16
    rows = query_nope.shape[0]
    share = stream.shape[0]
    sp, tp = lax.axis_index("sp"), lax.axis_index("tp")
    where = jnp.stack([tp // 2, tp % 2, sp // RING, sp % RING, sp * rows]).astype(jnp.int32)

    keys, half_keys, cosine, sine = call(
        keys_kernel,
        (
            jax.ShapeDtypeStruct((rows, 640), bf16),
            jax.ShapeDtypeStruct((rows // 2, 640), bf16),
            jax.ShapeDtypeStruct((ROPE // 2, rows), jnp.float32),
            jax.ShapeDtypeStruct((ROPE // 2, rows), jnp.float32),
        ),
        [],
        rows * 2048,
        rows * 2048,
        where,
        latent,
        jnp.transpose(rope_key),
        latent_gain[None, :],
        scalars=1,
    )
    queries = call(
        queries_kernel,
        jax.ShapeDtypeStruct((rows, 384), bf16),
        [],
        rows * 2048,
        rows * 2048,
        query_nope.reshape(rows, 2 * NOPE),
        jnp.transpose(query_rope, (1, 2, 0)).reshape(2 * ROPE, rows),
        cosine,
        sine,
    )
    kup = jnp.transpose(key_up, (1, 0, 2))
    vup = jnp.transpose(value_up, (1, 0, 2))
    near_keys, half_far = up_and_down(keys), two_up(half_keys)
    far_keys = jnp.concatenate([near_keys, half_far], axis=0)
    early_keys = jnp.concatenate([keys, near_keys], axis=0)
    late_keys = jnp.concatenate([half_far, other_core(far_keys)], axis=0)
    all_keys = (early_keys, late_keys)
    far_queries = [along_y(queries, s) for s in SHIFTS]

    scaled_weight = (out_weight.astype(jnp.float32) * out_gain[:, None]).astype(bf16)
    pack = jnp.concatenate([stream, scaled_weight], axis=0)
    packs = [pack] + [along_x(pack, s) for s in SHIFTS]

    hidden = ff_in.shape[1]
    weights = call(
        pack_kernel,
        jax.ShapeDtypeStruct((2 * hidden, 128), bf16),
        [],
        hidden * 128,
        hidden * 1024,
        ff_in,
        ff_out,
    )
    line_in, line_out = join([weights] + [along("a", weights, s) for s in SHIFTS])

    def spread(line):
        up, down = along("b", line, 1), along("b", line, 3)
        far_up = along("b", up[:2], 1)
        return line, up, down, far_up, along("b", down[2:], 3)

    in_lines, out_lines = spread(line_in), spread(line_out)

    backs = []
    for s, q in zip(SHIFTS, far_queries):
        backs.append(along_y(attend(q, all_keys, kup, vup), -s))
    mine = [attend(queries, (k,), kup, vup) for k in all_keys]
    head_out = call(
        combine_kernel,
        jax.ShapeDtypeStruct((rows, 256), bf16),
        [],
        rows * 256 * 16,
        rows * 384 * 2 * 6,
        *mine,
        *backs,
    )
    packs, _ = lax.optimization_barrier((packs, head_out))
    own_stream = jnp.concatenate([p[:share] for p in packs], axis=0)
    other_stream = other_core(own_stream)
    heads = [head_out] + [along_x(head_out, s) for s in SHIFTS]
    projected = call(
        project_kernel,
        jax.ShapeDtypeStruct((rows, 2176), bf16),
        [],
        2 * rows * 1024 * 2048,
        rows * 6400 + 1024 * 4096,
        *heads,
        *packs,
    )
    other_projected = other_core(projected)
    activation, mid_stream = call(
        ff_in_kernel,
        (
            jax.ShapeDtypeStruct((rows, ff_in.shape[1]), bf16),
            jax.ShapeDtypeStruct((share, stream.shape[1]), jnp.float32),
        ),
        [pltpu.VMEM((rows, 2048), bf16), pltpu.VMEM((rows, 2048), bf16)],
        2 * rows * 2048 * 1024,
        rows * 10000 + 2048 * 2048,
        where,
        projected,
        other_projected,
        own_stream,
        other_stream,
        norm_gain[None, :],
        *in_lines,
        scalars=1,
    )
    keep, send = call(
        ff_out_kernel,
        (
            jax.ShapeDtypeStruct((rows // 2, 2048), jnp.float32),
            jax.ShapeDtypeStruct((rows // 2, 2048), bf16),
        ),
        [],
        2 * rows * 2048 * hidden,
        rows * 5000 + 4096 * hidden,
        where,
        activation,
        *out_lines,
        scalars=1,
    )
    summed = keep + other_core(send).astype(jnp.float32)
    mixed = summed[0:share]
    for i, s in enumerate(SHIFTS):
        block = summed[(i + 1) * share : (i + 2) * share].astype(bf16)
        mixed = mixed + along_x(block, -s).astype(jnp.float32)
    return (mid_stream + mixed).astype(bf16)


def solution(mesh):
    placed = (
        P(("sp", "tp"), None),
        P("sp", "tp", None),
        P("sp", "tp", None),
        P("sp", None),
        P("sp", None),
        P(),
        P(None, "tp", None),
        P(None, "tp", None),
        P("tp"),
        P("tp", None),
        P(),
        P("sp", "tp"),
        P("tp", "sp"),
    )

    return jax.shard_map(
        body, mesh=mesh, in_specs=placed, out_specs=P(("sp", "tp"), None), check_vma=False
    )
```

```python
import functools
import math

import jax
import jax.numpy as jnp
import numpy as np
from jax import lax
from jax.experimental import pallas as pl
from jax.experimental.pallas import tpu as pltpu
from jax.sharding import PartitionSpec as P


HEADS = 16
NOPE = 128
ROPE = 64
LATENT = 512
VDIM = 128
RING = 4
SHARE = 48
SHIFTS = (1, 3, 2)

EPS = 1e-06
THETA = 10000.0
SCALE2 = math.log2(math.e) / math.sqrt(NOPE + ROPE)
LAST_LAST = (((1,), (1,)), ((), ()))


def sp_of(z, y):
    return (z % RING) * RING + (y % RING)


def along(line, values, shift):
    pairs = []
    for z in range(RING):
        for y in range(RING):
            for t in range(2 * RING):
                on_y = (line == "a") == (t % 2 == 0)
                to = sp_of(z, y + shift) if on_y else sp_of(z + shift, y)
                pairs.append((sp_of(z, y) * 2 * RING + t, to * 2 * RING + t))
    return lax.ppermute(values, ("sp", "tp"), pairs)


def along_y(values, shift):
    pairs = [(sp_of(z, y), sp_of(z, y + shift)) for z in range(RING) for y in range(RING)]
    return lax.ppermute(values, "sp", pairs)


def up_and_down(values):
    pairs = []
    for z in range(RING):
        for y in range(RING):
            for t in range(2 * RING):
                to = sp_of(z + (1 if t % 2 == 0 else -1), y)
                pairs.append((sp_of(z, y) * 2 * RING + t, to * 2 * RING + t))
    return lax.ppermute(values, ("sp", "tp"), pairs)


def two_up(values):
    pairs = [(sp_of(z, y), sp_of(z + 2, y)) for z in range(RING) for y in range(RING)]
    return lax.ppermute(values, "sp", pairs)


def along_x(values, shift):
    pairs = [(2 * x + c, 2 * ((x + shift) % RING) + c) for x in range(RING) for c in range(2)]
    return lax.ppermute(values, "tp", pairs)


def other_core(values):
    return lax.ppermute(values, "tp", [(t, t ^ 1) for t in range(2 * RING)])


def dot32(a, b, dims=None):
    if dims is None:
        return jnp.dot(a, b, preferred_element_type=jnp.float32)
    return lax.dot_general(a, b, dims, preferred_element_type=jnp.float32)


def call(kernel, outs, scratch, flops, moved, *args, scalars=0):
    vmem = pl.BlockSpec(memory_space=pltpu.VMEM)
    smem = pl.BlockSpec(memory_space=pltpu.SMEM)
    return pl.pallas_call(
        kernel,
        out_shape=outs,
        in_specs=[smem] * scalars + [vmem] * (len(args) - scalars),
        out_specs=jax.tree.map(lambda _: vmem, outs),
        scratch_shapes=scratch,
        compiler_params=pltpu.CompilerParams(vmem_limit_bytes=24 * 1024 * 1024),
        cost_estimate=pl.CostEstimate(flops=flops, bytes_accessed=moved, transcendentals=0),
    )(*args)


def join_kernel(a_ref, b_ref, c_ref, d_ref, in_ref, out_ref):
    hidden = in_ref.shape[1]
    for i, ref in enumerate((a_ref, b_ref, c_ref, d_ref)):
        out_ref[i] = ref[0:hidden, :]
        in_ref[i] = ref[hidden:, :]


def join(packs):
    hidden = packs[0].shape[0] // 2
    half = jax.ShapeDtypeStruct((4, hidden, 128), packs[0].dtype)
    moved = 32 * hidden * 128
    return call(join_kernel, (half, half), [], moved, moved, *packs)


def angles(start, rows):
    values = np.power(np.float32(THETA), -np.arange(0, ROPE, 2, dtype=np.float32) / ROPE)
    index = lax.broadcasted_iota(jnp.int32, (ROPE // 2, 1), 0)
    inverse = jnp.zeros((ROPE // 2, 1), jnp.float32)
    for i, value in enumerate(values):
        inverse = jnp.where(index == i, float(value), inverse)
    token = (start + lax.broadcasted_iota(jnp.int32, (1, rows), 1)).astype(jnp.float32)
    angle = inverse * token
    return jnp.cos(angle), jnp.sin(angle)


def rotated(ref, at, cosine, sine):
    pairs = ROPE // 2
    low = ref[at : at + pairs, :].astype(jnp.float32)
    high = ref[at + pairs : at + ROPE, :].astype(jnp.float32)
    return [low * cosine - high * sine, low * sine + high * cosine]


def keys_kernel(where_ref, latent_ref, key_ref, gain_ref, k_ref, half_ref, cos_ref, sin_ref):
    rows = k_ref.shape[0]
    cosine, sine = angles(where_ref[4], rows)
    cos_ref[...] = cosine
    sin_ref[...] = sine
    zeros = jnp.zeros((ROPE, rows), jnp.float32)
    keys = jnp.concatenate(rotated(key_ref, 0, cosine, sine) + [zeros], axis=0)
    k_ref[:, LATENT : LATENT + 128] = jnp.transpose(keys).astype(jnp.bfloat16)
    lat = latent_ref[...].astype(jnp.float32)
    mean = jnp.mean(lat * lat, axis=1, keepdims=True)
    k_ref[:, 0:LATENT] = (lat * lax.rsqrt(mean + EPS) * gain_ref[...]).astype(jnp.bfloat16)
    half = rows // 2
    half_ref[...] = k_ref[pl.ds(pl.multiple_of(where_ref[1] * half, 64), half), :]


def pack_kernel(in_ref, out_ref, pack_ref):
    hidden = out_ref.shape[0]
    pack_ref[0:hidden, :] = out_ref[...]
    for n in range(hidden // 128):
        pack_ref[hidden + n * 128 : hidden + (n + 1) * 128, :] = in_ref[:, n * 128 : (n + 1) * 128]


def queries_kernel(nope_ref, rope_ref, cos_ref, sin_ref, q_ref):
    cosine, sine = cos_ref[...], sin_ref[...]
    parts = rotated(rope_ref, 0, cosine, sine) + rotated(rope_ref, ROPE, cosine, sine)
    q_ref[:, 0:256] = nope_ref[...]
    q_ref[:, 256:384] = jnp.transpose(jnp.concatenate(parts, axis=0)).astype(jnp.bfloat16)


def attend_kernel(q_ref, kup_ref, vup_ref, *refs):
    key_refs, o_ref, qs = refs[:-2], refs[-2], refs[-1]
    rows = q_ref.shape[0]
    lane = lax.broadcasted_iota(jnp.int32, (rows, 128), 1)

    raw = []
    for h in range(2):
        rot = q_ref[:, 256:384].astype(jnp.float32)
        rot = pltpu.roll(rot, ROPE, 1) if h else rot
        qs[h, :, 512:640] = jnp.where(lane < ROPE, rot, 0.0).astype(jnp.bfloat16)
        cols = slice(h * 128, (h + 1) * 128)
        qs[h, :, 0:512] = dot32(q_ref[:, cols], kup_ref[h], LAST_LAST).astype(jnp.bfloat16)
    for h in range(2):
        raw.append([dot32(qs[h], k[...], LAST_LAST) for k in key_refs])
    stats = jnp.zeros((rows, 128), jnp.float32)
    for h, scores in enumerate(raw):
        tops = [jnp.max(part, axis=1, keepdims=True) for part in scores]
        top = functools.reduce(jnp.maximum, tops) * SCALE2
        total, out = 0.0, 0.0
        for part, k in zip(scores, key_refs):
            expo = jnp.exp2(part * SCALE2 - top)
            total += jnp.sum(expo, axis=1, keepdims=True)
            out += dot32(expo.astype(jnp.bfloat16), k[:, 0:512])
        out = (out / total).astype(jnp.bfloat16)
        o_ref[0:rows, h * 128 : (h + 1) * 128] = dot32(out, vup_ref[h]).astype(jnp.bfloat16)
        lse = top + jnp.log2(total)
        high = lse.astype(jnp.bfloat16).astype(jnp.float32)
        mid = (lse - high).astype(jnp.bfloat16).astype(jnp.float32)
        low = lse - high - mid
        stats = jnp.where(lane == 3 * h, high, stats)
        stats = jnp.where(lane == 3 * h + 1, mid, stats)
        stats = jnp.where(lane == 3 * h + 2, low, stats)
    flat = jnp.transpose(stats)[0:8]
    rest = jnp.concatenate([flat[:, 256:384], jnp.zeros((8, 128), jnp.float32)], axis=1)
    o_ref[rows : rows + 16, :] = jnp.concatenate([flat[:, 0:256], rest], axis=0).astype(jnp.bfloat16)


def attend(queries, keys, kup, vup):
    rows = queries.shape[0]
    count = sum(k.shape[0] for k in keys)
    return call(
        attend_kernel,
        jax.ShapeDtypeStruct((rows + 16, 256), jnp.bfloat16),
        [pltpu.VMEM((2, rows, 640), jnp.bfloat16)],
        2 * 2 * rows * count * 1280,
        count * 1280 + rows * 1536,
        queries,
        kup,
        vup,
        *keys,
    )


def combine_kernel(*refs):
    parts, h_ref = refs[:-1], refs[-1]
    rows = h_ref.shape[0]
    lane = lax.broadcasted_iota(jnp.int32, (rows, 128), 1)
    stats = []
    for ref in parts:
        tail = ref[rows : rows + 16, :].astype(jnp.float32)
        flat = jnp.concatenate([tail[0:8], tail[8:16, 0:128]], axis=1)
        flat = jnp.concatenate([flat, jnp.zeros((120, rows), jnp.float32)], axis=0)
        stats.append(jnp.transpose(flat))
    for h in range(2):
        mine = (lane >= 3 * h) & (lane < 3 * h + 3)
        lses = [jnp.sum(jnp.where(mine, s, 0.0), axis=1, keepdims=True) for s in stats]
        top = functools.reduce(jnp.maximum, lses)
        shares = [jnp.exp2(v - top) for v in lses]
        whole = sum(shares)
        cols = slice(h * 128, (h + 1) * 128)
        summed = sum(s * ref[0:rows, cols].astype(jnp.float32) for s, ref in zip(shares, parts))
        h_ref[:, cols] = (summed / whole).astype(jnp.bfloat16)


def project_kernel(h0, h1, h2, h3, w0, w1, w2, w3, out_ref):
    heads = (h0, h1, h2, h3)
    rows = h0.shape[0]
    for n in range(4):
        cols = slice(n * 512, (n + 1) * 512)
        total = sum(
            dot32(h[...], w[SHARE : SHARE + 256, cols]) for h, w in zip(heads, (w0, w1, w2, w3))
        )
        out_ref[:, cols] = total.astype(jnp.bfloat16)
    squares = sum(
        jnp.sum(jnp.square(h[...].astype(jnp.float32)), axis=1, keepdims=True) for h in heads
    )
    high = squares.astype(jnp.bfloat16).astype(jnp.float32)
    mid = (squares - high).astype(jnp.bfloat16).astype(jnp.float32)
    low = squares - high - mid
    lane = lax.broadcasted_iota(jnp.int32, (rows, 128), 1)
    stats = jnp.where(lane == 0, high, jnp.where(lane == 1, mid, jnp.where(lane == 2, low, 0.0)))
    out_ref[:, 2048:2176] = stats.astype(jnp.bfloat16)


def ff_in_kernel(
    where_ref, own_ref, oth_ref, sa_ref, sb_ref, gain_ref, w0, w1, w2, w3a, w3b,
    act_ref, mid_ref, xs, xr,
):
    share = mid_ref.shape[0]
    x, c = where_ref[0], where_ref[1]
    gain = gain_ref[...]
    for i in range(8):
        shift = (0, *SHIFTS)[i % 4]
        core = c if i < 4 else 1 - c
        block = lax.rem(x + RING - shift, RING) * 2 + core
        rows = pl.ds(pl.multiple_of(block * share, 16), share)
        both = own_ref[rows, :].astype(jnp.float32) + oth_ref[rows, :].astype(jnp.float32)
        squares = jnp.sum(both[:, 2048:2176], axis=1, keepdims=True)
        scale = lax.rsqrt(squares / (HEADS * VDIM) + EPS)
        at = (i % 4) * share
        stream = (sa_ref if i < 4 else sb_ref)[at : at + share, :]
        mid = stream.astype(jnp.float32) + scale * both[:, 0:2048]
        if i == 0:
            mid_ref[...] = mid
        mean = jnp.mean(mid * mid, axis=1, keepdims=True)
        xs[i * share : (i + 1) * share, :] = (mid * lax.rsqrt(mean + EPS) * gain).astype(jnp.bfloat16)
    for i, block in enumerate(blocks_of(where_ref)):
        cols = pl.ds(pl.multiple_of(block * 128, 128), 128)
        xr[:, i * 128 : (i + 1) * 128] = xs[:, cols]
    hidden = act_ref.shape[1]
    pieces = [(w, k) for w in (w0, w1, w2, w3a, w3b) for k in range(w.shape[0])]
    for n in range(0, hidden // 128, 2):
        columns = []
        for m in (n, n + 1):
            at = m * 128
            columns.append(jnp.concatenate([w[k, at : at + 128, :] for w, k in pieces], axis=0))
        total = dot32(xr[...], jnp.concatenate(columns, axis=1))
        act_ref[:, n * 128 : (n + 2) * 128] = jnp.square(jnp.maximum(total, 0.0)).astype(jnp.bfloat16)


def blocks_of(where_ref):
    core, z, y = where_ref[1], where_ref[2], where_ref[3]
    order = (0, *SHIFTS)
    blocks = []
    for outer in order:
        for inner in order:
            dz = jnp.where(core == 0, outer, inner)
            dy = jnp.where(core == 0, inner, outer)
            blocks.append(lax.rem(z + RING - dz, RING) * RING + lax.rem(y + RING - dy, RING))
    return blocks


def ff_out_kernel(where_ref, act_ref, w0, w1, w2, w3a, w3b, keep_ref, send_ref):
    half = keep_ref.shape[0]
    hidden = act_ref.shape[1]
    blocks = blocks_of(where_ref)
    pieces = [(w, k) for w in (w0, w1, w2, w3a, w3b) for k in range(w.shape[0])]
    for i in range(0, len(pieces), 2):
        both = jnp.concatenate([w[k, 0:hidden, :] for w, k in pieces[i : i + 2]], axis=1)
        out = dot32(act_ref[...], both)
        for k in range(2):
            cols = pl.ds(pl.multiple_of(blocks[i + k] * 128, 128), 128)
            keep_ref[:, cols] = out[0:half, k * 128 : (k + 1) * 128]
            send_ref[:, cols] = out[half:, k * 128 : (k + 1) * 128].astype(jnp.bfloat16)


def body(
    stream,
    query_nope,
    query_rope,
    latent,
    rope_key,
    latent_gain,
    key_up,
    value_up,
    out_gain,
    out_weight,
    norm_gain,
    ff_in,
    ff_out,
):
    bf16 = jnp.bfloat16
    rows = query_nope.shape[0]
    share = stream.shape[0]
    sp, tp = lax.axis_index("sp"), lax.axis_index("tp")
    where = jnp.stack([tp // 2, tp % 2, sp // RING, sp % RING, sp * rows]).astype(jnp.int32)

    keys, half_keys, cosine, sine = call(
        keys_kernel,
        (
            jax.ShapeDtypeStruct((rows, 640), bf16),
            jax.ShapeDtypeStruct((rows // 2, 640), bf16),
            jax.ShapeDtypeStruct((ROPE // 2, rows), jnp.float32),
            jax.ShapeDtypeStruct((ROPE // 2, rows), jnp.float32),
        ),
        [],
        rows * 2048,
        rows * 2048,
        where,
        latent,
        jnp.transpose(rope_key),
        latent_gain[None, :],
        scalars=1,
    )
    queries = call(
        queries_kernel,
        jax.ShapeDtypeStruct((rows, 384), bf16),
        [],
        rows * 2048,
        rows * 2048,
        query_nope.reshape(rows, 2 * NOPE),
        jnp.transpose(query_rope, (1, 2, 0)).reshape(2 * ROPE, rows),
        cosine,
        sine,
    )
    kup = jnp.transpose(key_up, (1, 0, 2))
    vup = jnp.transpose(value_up, (1, 0, 2))
    near_keys, half_far = up_and_down(keys), two_up(half_keys)
    far_keys = jnp.concatenate([near_keys, half_far], axis=0)
    early_keys = jnp.concatenate([keys, near_keys], axis=0)
    late_keys = jnp.concatenate([half_far, other_core(far_keys)], axis=0)
    all_keys = (early_keys, late_keys)
    far_queries = [along_y(queries, s) for s in SHIFTS]

    scaled_weight = (out_weight.astype(jnp.float32) * out_gain[:, None]).astype(bf16)
    pack = jnp.concatenate([stream, scaled_weight], axis=0)
    packs = [pack] + [along_x(pack, s) for s in SHIFTS]

    hidden = ff_in.shape[1]
    weights = call(
        pack_kernel,
        jax.ShapeDtypeStruct((2 * hidden, 128), bf16),
        [],
        hidden * 128,
        hidden * 1024,
        ff_in,
        ff_out,
    )
    line_in, line_out = join([weights] + [along("a", weights, s) for s in SHIFTS])

    def spread(line):
        up, down = along("b", line, 1), along("b", line, 3)
        far_up = along("b", up[:2], 1)
        return line, up, down, far_up, along("b", down[2:], 3)

    in_lines, out_lines = spread(line_in), spread(line_out)

    backs = []
    for s, q in zip(SHIFTS, far_queries):
        backs.append(along_y(attend(q, all_keys, kup, vup), -s))
    mine = [attend(queries, (k,), kup, vup) for k in all_keys]
    head_out = call(
        combine_kernel,
        jax.ShapeDtypeStruct((rows, 256), bf16),
        [],
        rows * 256 * 16,
        rows * 384 * 2 * 6,
        *mine,
        *backs,
    )
    packs, _ = lax.optimization_barrier((packs, head_out))
    own_stream = jnp.concatenate([p[:share] for p in packs], axis=0)
    other_stream = other_core(own_stream)
    heads = [head_out] + [along_x(head_out, s) for s in SHIFTS]
    projected = call(
        project_kernel,
        jax.ShapeDtypeStruct((rows, 2176), bf16),
        [],
        2 * rows * 1024 * 2048,
        rows * 6400 + 1024 * 4096,
        *heads,
        *packs,
    )
    other_projected = other_core(projected)
    activation, mid_stream = call(
        ff_in_kernel,
        (
            jax.ShapeDtypeStruct((rows, ff_in.shape[1]), bf16),
            jax.ShapeDtypeStruct((share, stream.shape[1]), jnp.float32),
        ),
        [pltpu.VMEM((rows, 2048), bf16), pltpu.VMEM((rows, 2048), bf16)],
        2 * rows * 2048 * 1024,
        rows * 10000 + 2048 * 2048,
        where,
        projected,
        other_projected,
        own_stream,
        other_stream,
        norm_gain[None, :],
        *in_lines,
        scalars=1,
    )
    keep, send = call(
        ff_out_kernel,
        (
            jax.ShapeDtypeStruct((rows // 2, 2048), jnp.float32),
            jax.ShapeDtypeStruct((rows // 2, 2048), bf16),
        ),
        [],
        2 * rows * 2048 * hidden,
        rows * 5000 + 4096 * hidden,
        where,
        activation,
        *out_lines,
        scalars=1,
    )
    summed = keep + other_core(send).astype(jnp.float32)
    mixed = summed[0:share]
    for i, s in enumerate(SHIFTS):
        block = summed[(i + 1) * share : (i + 2) * share].astype(bf16)
        mixed = mixed + along_x(block, -s).astype(jnp.float32)
    return (mid_stream + mixed).astype(bf16)


def solution(mesh):
    placed = (
        P(("sp", "tp"), None),
        P("sp", "tp", None),
        P("sp", "tp", None),
        P("sp", None),
        P("sp", None),
        P(),
        P(None, "tp", None),
        P(None, "tp", None),
        P("tp"),
        P("tp", None),
        P(),
        P("sp", "tp"),
        P("tp", "sp"),
    )

    return jax.shard_map(
        body, mesh=mesh, in_specs=placed, out_specs=P(("sp", "tp"), None), check_vma=False
    )
```
